32 devices in a mesh: sp: 16 (over z, y, x), tp: 2 (over core).
Axes of the slice: x: 2, y: 2, z: 4, core: 2. Of those that a mesh axis runs over, the one named last changes fastest.
Arguments:
- tokens: bfloat16 [4096, 4096], P('sp'), may hold values from -5 to 5
- documents: int32 [4096], P('sp'), may hold values from 0 to 3, never falling along the last dimension, each value on 1 to 2048 neighbouring positions
- norm_gain: float32 [2, 4096], replicated, may hold values from 0.1 to 1.9
- in_weight: bfloat16 [2, 4096, 2048], P(None, 'sp', 'tp'), may hold values from -0.09375 to 0.09375
- conv_taps: float32 [2, 4, 2048], P(None, None, 'tp'), may hold values from -3 to 3
- conv_bias: float32 [2, 2048], P(None, 'tp'), may hold values from -0.75 to 0.75
- recur_gate: bfloat16 [2, 32, 64, 64], P(None, 'tp'), may hold values from -0.75 to 0.75
- input_gate: bfloat16 [2, 32, 64, 64], P(None, 'tp'), may hold values from -0.75 to 0.75
- recur_bias: float32 [2, 2048], P(None, 'tp'), may hold values from -4 to 4
- input_bias: float32 [2, 2048], P(None, 'tp'), may hold values from -4 to 4
- decay_param: float32 [2, 2048], P(None, 'tp'), may hold values from 4 to 7
- out_weight: bfloat16 [2, 2048, 4096], P(None, 'tp', 'sp'), may hold values from -0.375 to 0.375
Outputs:
- layered: bfloat16 [4096, 4096], P('sp')
The draws below stay inside these ranges and needn't reach their ends.
All inputs are finite; a program needn't handle non-finite values.
Results may differ from the reference program's by a relative error of at most 0.017.
Values may be sent and summed in bfloat16 or wider, within the bound.
A program may use at most 128 MiB of HBM per device.

```python
import math
import jax
import jax.numpy as jnp
import numpy as np
from jax import lax

D = 4096
RW = 2048
BD = 64
K = 4
LAYERS = 2
TOK_DEV = 256
TOKENS = 4096
NB = 32
N_SP = 16
N_TP = 2


def draw_tokens(key, part):
    scale_key, value_key, mean_key = jax.random.split(jax.random.fold_in(key, 11), 3)
    log_scale = jax.random.uniform(scale_key, (TOKENS // 128, 1), jnp.float32, -1.3863, -0.2877)
    block_scale = jnp.repeat(jnp.exp(log_scale), 128, axis=0)
    base = jax.random.normal(value_key, (TOKENS, D), jnp.float32)
    base = jnp.clip(base, -6.0, 6.0)
    return (base * block_scale).astype(jnp.bfloat16)


def draw_decay_param(key, part):
    flag_key, slow_key, fast_key = jax.random.split(jax.random.fold_in(key, 23), 3)
    picked = jax.random.randint(flag_key, (LAYERS, RW), 0, 2)
    slow_value = jax.random.uniform(slow_key, (LAYERS, RW), jnp.float32, 6.5, 7.0)
    fast_value = jax.random.uniform(fast_key, (LAYERS, RW), jnp.float32, 4.0, 5.0)
    return jnp.where(picked == 0, fast_value, slow_value)


def shard_levels(own_key, extent, pieces, smallest, high):
    gain = 1.0
    for dim, parts in pieces:
        draws = jax.random.uniform(jax.random.fold_in(jax.random.fold_in(own_key, 6), dim), (parts,), jnp.float32, smallest / len(pieces), high / len(pieces))
        gain = gain * jnp.repeat(jnp.exp(draws), extent[dim] // parts).reshape((-1,) + (1,) * (len(extent) - 1 - dim))
    return gain


def split_up(number_of, total, bound, lean):
    portions = [(1 << 20) // math.isqrt(standing ** lean) + 1 for standing in range(2, number_of + 1)]
    surplus, holding = total - bound - (number_of - 1), [1] * (number_of - 1)
    while surplus > 0:
        movable = [i for i in range(number_of - 1) if holding[i] < bound]
        mass, budget = sum([portions[i] for i in movable]), surplus
        for i in movable:
            addition = min(bound - holding[i], max(1, budget * portions[i] // mass), surplus)
            holding[i] = holding[i] + addition
            surplus = surplus - addition
    return np.array([bound] + holding)


def ragged(rng, number_of, total, most, slope):
    if number_of == 2:
        one = jax.random.randint(rng, (), max(1, total - most), min(most, total - 1) + 1)
        return jnp.stack([one, total - one])
    lengths = jnp.asarray(split_up(number_of, total, most, slope), jnp.int32)
    twos = (number_of - 1) // 2
    donor, sink = lengths[1:1 + 2 * twos:2], lengths[2:2 + 2 * twos:2]
    margin = jnp.minimum(donor - 1, most - sink)
    moved = jax.random.randint(jax.random.fold_in(rng, 1), (twos,), 0, 1 << 20) % (margin + 1)
    lengths = lengths.at[1:1 + 2 * twos:2].set(donor - moved).at[2:2 + 2 * twos:2].set(sink + moved)
    return lengths[jax.random.permutation(jax.random.fold_in(rng, 2), number_of)]


def bell_draw(rng, shape, scale, most, shards=(), kind=jnp.bfloat16):
    drawn = jax.random.normal(rng, shape, jnp.float32) * scale
    if len(shards) > 0:
        drawn = shard_levels(rng, shape, shards, -0.22, 0.18) * drawn
    return jnp.clip(drawn, min=-most, max=most).astype(kind)


def setup_inputs(seed: int = 0) -> dict:
    splits = jax.random.split(jax.random.key(seed), 13)
    tokens = draw_tokens(jax.random.fold_in(splits[12], 71), 0)
    documents = jnp.searchsorted(jnp.cumsum(ragged(splits[1], N_SP // 4, TOKENS, 8 * TOK_DEV, 0)), jnp.arange(TOKENS), side="right").astype(jnp.int32)
    norm_gain = jnp.clip(1.0 + 0.18 * jax.random.normal(splits[2], (LAYERS, D), jnp.float32), 0.1, 1.9)
    in_weight = bell_draw(splits[3], (LAYERS, D, RW), D ** -0.5, 0.09375, ((1, 16), (2, 2)))
    conv_taps = bell_draw(splits[4], (LAYERS, K, RW), K ** -0.5, 3.0, ((2, 2),), jnp.float32)
    conv_bias = bell_draw(splits[5], (LAYERS, RW), 0.05, 0.75, ((1, 2),), jnp.float32)
    recur_gate = bell_draw(splits[6], (LAYERS, NB, BD, BD), BD ** -0.5, 0.75, ((1, 2),))
    input_gate = bell_draw(splits[7], (LAYERS, NB, BD, BD), BD ** -0.5, 0.75, ((1, 2),))
    recur_bias = bell_draw(splits[8], (LAYERS, RW), 1.0, 4.0, ((1, 2),), jnp.float32)
    input_bias = bell_draw(splits[9], (LAYERS, RW), 1.0, 4.0, ((1, 2),), jnp.float32)
    decay_param = draw_decay_param(jax.random.fold_in(splits[12], 71), 0)
    out_weight = bell_draw(splits[11], (LAYERS, RW, D), (RW // 8) ** -0.5, 0.375, ((1, 2), (2, 16)))
    return {"tokens": tokens, "documents": documents, "norm_gain": norm_gain, "in_weight": in_weight, "conv_taps": conv_taps, "conv_bias": conv_bias, "recur_gate": recur_gate, "input_gate": input_gate, "recur_bias": recur_bias, "input_bias": input_bias, "decay_param": decay_param, "out_weight": out_weight}


RG_C = 8.0
EPS = 0.1

def norm_rows(values_in, gain_row):
    values = values_in.astype(jnp.float32)
    scaled = values * lax.rsqrt(lax.optimization_barrier(jnp.mean(values * values, axis=-1, keepdims=True)) + EPS)
    return (scaled * gain_row[None, :]).astype(jnp.bfloat16)

def combine(earlier, following):
    return (earlier[0] * following[0], following[0] * earlier[1] + following[1])

def reference(tokens, documents, norm_gain, in_weight, conv_taps, conv_bias, recur_gate, input_gate, recur_bias, input_bias, decay_param, out_weight):
    state_x = tokens
    prev_doc = jnp.concatenate([documents[:1], documents[:-1]])
    reset = documents != prev_doc
    group_width = RW // N_TP
    for depth_at in range(LAYERS):
        normed = norm_rows(state_x, norm_gain[depth_at])
        mixed_in = jnp.dot(normed, in_weight[depth_at], preferred_element_type=jnp.float32).astype(jnp.bfloat16)
        values_in = mixed_in.astype(jnp.float32)
        conv_sum = conv_bias[depth_at][None, :] + conv_taps[depth_at, 0][None, :] * values_in
        for lag_step in range(1, K):
            shifted = jnp.concatenate([jnp.zeros((lag_step, RW), jnp.float32), values_in[:-lag_step]], axis=0)
            shifted_doc = jnp.concatenate([jnp.full((lag_step,), -1, jnp.int32), documents[:-lag_step]], axis=0)
            same_doc = (shifted_doc == documents)[:, None]
            conv_sum = conv_sum + jnp.where(same_doc, conv_taps[depth_at, lag_step][None, :] * shifted, 0.0)
        conv_out = conv_sum.astype(jnp.bfloat16)
        grouped = conv_out.astype(jnp.float32).reshape(TOKENS, NB, BD)
        recur_rate = jax.nn.sigmoid(jnp.einsum('snb,nbc->snc', grouped, recur_gate[depth_at].astype(jnp.float32)).reshape(TOKENS, RW) + recur_bias[depth_at][None, :])
        input_rate = jax.nn.sigmoid(jnp.einsum('snb,nbc->snc', grouped, input_gate[depth_at].astype(jnp.float32)).reshape(TOKENS, RW) + input_bias[depth_at][None, :])
        log_decay = -RG_C * jax.nn.softplus(-decay_param[depth_at])[None, :] * recur_rate
        decay_now = jnp.where(reset[:, None], 0.0, jnp.exp(log_decay))
        drive_term = jnp.sqrt(jnp.maximum(-jnp.expm1(2.0 * log_decay), 0.0)) * (input_rate * conv_out.astype(jnp.float32))
        _, states = lax.associative_scan(combine, (decay_now, drive_term), axis=0)
        hidden = states.astype(jnp.bfloat16)
        summed = jnp.zeros((TOKENS, D), jnp.float32)
        for group in range(N_TP):
            low = group * group_width
            partial_term = jnp.dot(hidden[:, low:low + group_width], out_weight[depth_at, low:low + group_width], preferred_element_type=jnp.float32).astype(jnp.bfloat16)
            partial_term = lax.optimization_barrier(partial_term)
            summed = summed + partial_term.astype(jnp.float32)
        state_x = (state_x.astype(jnp.float32) + summed).astype(jnp.bfloat16)
    return state_x
```

```python
import functools

import jax
import jax.numpy as jnp
from jax import lax
from jax.experimental import pallas as pl
from jax.experimental.pallas import tpu as pltpu
from jax.sharding import PartitionSpec as P

RG_C = 8.0
EPS = 0.1
G = 4
MESH = pl.DeviceIdType.MESH
F32 = jnp.float32
BF16 = jnp.bfloat16
VM = pl.BlockSpec(memory_space=pltpu.VMEM)


def send(src, dst, send_sem, recv_sem, **device):
    return pltpu.make_async_remote_copy(
        src_ref=src,
        dst_ref=dst,
        send_sem=send_sem,
        recv_sem=recv_sem,
        device_id=device,
        device_id_type=MESH,
    )


def minus_expm1(x):
    series = 1.0 + x * (1.0 / 8.0)
    for n in range(7, 1, -1):
        series = 1.0 + (x * (1.0 / n)) * series
    return jnp.where(x > -0.5, -x * series, 1.0 - jnp.exp(x))


def flip(i, m):
    return 2 * lax.rem(i // 2 + m // 2, 2) + lax.rem(i + m, 2)


def member(square, o, j):
    if square:
        return (o // 2) * 8 + (j // 2) * 4 + (o % 2) * 2 + j % 2
    return o * G + j


def whole_kernel(
    n_sp, n_tp, square,
    x_in, win_in, wout_in, doc_ref, gain_ref, taps_ref, bias_ref, rbias_ref, ibias_ref, decay_ref,
    rgate_ref, igate_ref,
    o_ref,
    xbuf, win, wout, part, gotten, sq_out, sq_got, tails, tail_out, doc_tail, docs, gain, coef,
    ext, a_buf, b_buf, ends, hid, psend, pgot,
    own_sem, x_own, x_send, x_recv, xt_send, xt_recv, w_send, w_recv, doc_sem, rs_send, rs_recv,
    sq_send, sq_recv, tail_sem, end_send, end_recv, ag_send, ag_recv, tp_send, tp_recv, f_send,
    f_recv, ft_send, ft_recv,
):
    g = G
    me = lax.axis_index("sp")
    core = lax.axis_index("tp")
    outer = n_sp // g
    if square:
        inner = 2 * lax.rem(me // 4, 2) + lax.rem(me, 2)
        place = 2 * (me // 8) + lax.rem(me // 2, 2)
    else:
        inner, place = lax.rem(me, g), me // g
    near = {m: flip(inner, m) for m in (1, 2, 3)}
    at_sp = {m: member(square, place, near[m]) for m in (1, 2, 3)}
    layers, width, chans = win_in.shape
    rows, features = xbuf.shape[1], xbuf.shape[2] * g
    taps = taps_ref.shape[1]
    halves, span = hid.shape[0], hid.shape[3]
    half = rows // n_tp
    mine = pl.ds(core * half, half)
    strided = len(x_in.shape) == 2
    pieces = outer if strided else 1
    after = lax.rem(me + 1, n_sp)
    not_last, not_first = me < n_sp - 1, me > 0
    r0, r1 = pl.ds(0, rows // 2), pl.ds(rows // 2, rows - rows // 2)

    def piece(ref, at, j, o):
        if strided:
            return ref.at[at, pl.ds(pl.multiple_of(member(square, o, j) * width, width), width)]
        return ref.at[j, at, :]

    def slot(ref, j, at, o):
        return ref.at[j, at, pl.ds(o * width, width)] if strided else ref.at[j, at, :]

    def wref(l, kind, q):
        if kind == 0:
            return win_in.at[l, :, pl.ds(q * span, span)]
        return wout_in.at[l, pl.ds(q * span, span), :]

    def wslot(l, kind, q, o):
        if kind == 0:
            return win.at[l, pl.ds(o * width, width), pl.ds(q * span, span)]
        return wout.at[l, o, pl.ds(q * span, span), :]

    def weight_own(l, kind, q):
        return pltpu.make_async_copy(
            wref(l, kind, q), wslot(l, kind, q, place), own_sem.at[2 * l + kind, q]
        )

    def weight_copy(l, kind, q, to, src, o, sem, landed):
        k = 2 * l + kind
        return send(
            src, wslot(l, kind, q, o), w_send.at[k, q, sem], w_recv.at[k, q, landed],
            sp=member(square, to, inner),
        )

    def weight_copies(l, kind, q):
        own = wref(l, kind, q)
        if square:
            return [
                weight_copy(l, kind, q, flip(place, m), own, place, s, s)
                for s, m in enumerate((2, 1))
            ]
        copies = []
        for step in range(1, outer):
            to = lax.rem(place + step, outer)
            copies.append(weight_copy(l, kind, q, to, own, place, to, place))
        return copies

    def weight_go(l, kind, q):
        for copy in weight_copies(l, kind, q):
            copy.start()

    def weight_forward(l, kind, q):
        o = flip(place, 2)
        return weight_copy(l, kind, q, flip(place, 1), wslot(l, kind, q, o), o, 2, 2)

    def weight_arrived(l, kind, q, o, sem):
        weight_copy(l, kind, q, flip(place, 1), wslot(l, kind, q, o), o, 0, sem).wait_recv()

    def weight_relay(l, kind, q):
        if square:
            weight_arrived(l, kind, q, flip(place, 2), 0)
            weight_forward(l, kind, q).start()

    def weight_wait(l, kind, q):
        weight_own(l, kind, q).wait()
        if square:
            weight_arrived(l, kind, q, flip(place, 1), 1)
            weight_arrived(l, kind, q, flip(place, 3), 2)
        else:
            for step in range(1, outer):
                o = lax.rem(place + step, outer)
                src = wref(l, kind, q)
                weight_copy(l, kind, q, o, src, o, o, o).wait_recv()

    def weight_close(l, kind, q):
        for copy in weight_copies(l, kind, q):
            copy.wait_send()
        if square:
            weight_forward(l, kind, q).wait_send()

    def x_copy(m, o, landed):
        j = flip(inner, m)
        return send(
            piece(x_in, mine, j, o),
            slot(xbuf, landed, mine, o),
            x_send.at[m, o],
            x_recv.at[m, o],
            sp=member(square, place, j),
        )

    def own_piece(o):
        everything = pl.ds(0, rows)
        return pltpu.make_async_copy(
            piece(x_in, everything, inner, o), slot(xbuf, inner, everything, o), x_own.at[o]
        )

    weight_go(0, 0, 0)

    def x_go(step, _):
        for o in range(pieces):
            x_copy(g - step, o, inner).start()
        return 0

    lax.fori_loop(1, g, x_go, 0)
    for q in range(1, halves):
        weight_go(0, 0, q)
    for o in range(pieces):
        own_piece(o).start()
    for l in range(layers):
        for kind in range(2):
            for q in range(halves):
                weight_own(l, kind, q).start()

    column = jnp.broadcast_to(doc_ref[...].astype(F32), (128, rows))
    docs[pl.ds(8, rows), :] = jnp.transpose(column)
    doc_copy = send(
        docs.at[pl.ds(rows, 8)], doc_tail, doc_sem.at[0], doc_sem.at[1], sp=after
    )
    pl.when(not_last)(doc_copy.start)

    @pl.when(me == 0)
    def _():
        doc_tail[...] = jnp.full(doc_tail.shape, -1.0, F32)
        tails[...] = jnp.zeros(tails.shape, BF16)

    coef[...] = -RG_C * jax.nn.softplus(-decay_ref[...])
    if strided:
        for o in range(outer):
            at = pl.ds(pl.multiple_of(member(square, o, inner) * width, width), width)
            gain[:, pl.ds(o * width, width)] = gain_ref[:, at]
    else:
        gain[...] = gain_ref[...]

    def x_share(j, other, at):
        peer = lax.rem(core + other, n_tp)
        return send(
            xbuf.at[j, at], xbuf.at[j, at], xt_send.at[j, other - 1],
            xt_recv.at[j, n_tp - other - 1], tp=peer,
        )

    def x_arrive(m, _):
        j = flip(inner, m)
        for o in range(pieces):
            x_copy(m, o, j).wait_recv()
        for other in range(1, n_tp):
            x_share(j, other, mine).start()
        return 0

    lax.fori_loop(1, g, x_arrive, 0)
    for o in range(pieces):
        own_piece(o).wait()
    weight_relay(0, 0, 0)

    pl.when(not_first)(doc_copy.wait_recv)
    docs[pl.ds(0, 8), :] = doc_tail[...]

    def x_shared(m, _):
        j = flip(inner, m)
        for other in range(1, n_tp):
            peer = lax.rem(core + other, n_tp)
            at = pl.ds(peer * half, half)
            send(
                xbuf.at[j, at], xbuf.at[j, at], xt_send.at[j, other - 1],
                xt_recv.at[j, other - 1], tp=peer,
            ).wait_recv()
            x_share(j, other, mine).wait_send()
        for o in range(pieces):
            x_copy(m, o, inner).wait_send()
        return 0

    lax.fori_loop(1, g, x_shared, 0)
    pl.when(not_last)(doc_copy.wait_send)

    pair = 128
    dim = rgate_ref.shape[2]
    repeat = (
        lax.rem(lax.broadcasted_iota(jnp.int32, (dim, pair), 1), dim)
        == lax.broadcasted_iota(jnp.int32, (dim, pair), 0)
    ).astype(F32).astype(BF16)
    on_block = (
        lax.broadcasted_iota(jnp.int32, (pair, pair), 0) // dim
        == lax.broadcasted_iota(jnp.int32, (pair, pair), 1) // dim
    )

    def diagonal(ref, l, col):
        wide = jnp.dot(ref[l, pl.ds(col, pair), :], repeat, preferred_element_type=F32)
        return jnp.where(on_block, wide, 0.0).astype(BF16)

    sub = rows // 8
    lanes = span // pair

    def rs_copy(h, s):
        j, at, lands, to = (
            (3, r0, 2, 1), (3, r1, 2, 2), (1, r0, 0, 1), (2, r1, 1, 2), (2, r0, 1, 2),
            (1, r1, 0, 1),
        )[s]
        return send(
            part.at[h, near[j], at], gotten.at[h, lands, at], rs_send.at[h, s],
            rs_recv.at[h, s], sp=at_sp[to],
        )

    def ag_copy(h, s):
        j, at, to = (
            (0, r0, 1), (0, r1, 2), (0, r1, 1), (0, r0, 2), (1, r0, 2), (2, r1, 1),
        )[s]
        ref = hid.at[h, near[j] if j else inner, at]
        return send(ref, ref, ag_send.at[h, s], ag_recv.at[h, s], sp=at_sp[to])

    def ag_arrived(h, s):
        j, at = ((1, r0), (2, r1), (1, r1), (2, r0), (3, r0), (3, r1))[s]
        ref = hid.at[h, near[j], at]
        send(ref, ref, ag_send.at[h, s], ag_recv.at[h, s], sp=at_sp[1]).wait_recv()

    def sq_copy(l, m):
        return send(
            sq_out.at[near[m]], sq_got.at[m - 1], sq_send.at[m - 1], sq_recv.at[m - 1],
            sp=at_sp[m],
        )

    for l in range(layers):
        last = l == layers - 1

        for h in range(halves):
            weight_wait(l, 0, h)

            def project(step, _):
                m = jnp.where(step < 2, 3 - 2 * step, 6 - 2 * step)
                j = flip(inner, m)
                if h == 0:
                    x = xbuf[j].astype(F32)
                    squares = jnp.sum(x * x, axis=1, keepdims=True)
                    sq_out[j] = jnp.transpose(jnp.broadcast_to(squares, (rows, 128)))[0:8]
                    for n in (1, 2, 3):
                        pl.when(m == n)(sq_copy(l, n).start)
                    psend[j] = (x * gain[l : l + 1, :]).astype(BF16)
                out = jnp.dot(
                    psend[j], win[l, :, h * span : (h + 1) * span], preferred_element_type=F32
                )
                part[h, j] = out.astype(BF16)

                @pl.when(step == 0)
                def _():
                    rs_copy(h, 0).start()
                    rs_copy(h, 1).start()

                pl.when(step == 1)(rs_copy(h, 2).start)
                pl.when(step == 2)(rs_copy(h, 3).start)
                return 0

            lax.fori_loop(0, g, project, 0)
            if l == 0 and h + 1 < halves:
                weight_relay(0, 0, h + 1)
        for q in range(halves):
            if l == 0:
                weight_go(0, 1, q)

        for h in range(halves):
            rs_copy(h, 0).wait_recv()
            part[h, near[2], r0] = (
                part[h, near[2], r0].astype(F32) + gotten[h, 2, r0].astype(F32)
            ).astype(BF16)
            rs_copy(h, 4).start()
            rs_copy(h, 1).wait_recv()
            part[h, near[1], r1] = (
                part[h, near[1], r1].astype(F32) + gotten[h, 2, r1].astype(F32)
            ).astype(BF16)
            rs_copy(h, 5).start()

        scale = []
        tail_copies, prefixes = [], []

        def end_copy(h, dst, src):
            return send(
                ends.at[l, h, me], ends.at[l, h, src], end_send.at[l, h, dst],
                end_recv.at[l, h, src], sp=dst,
            )

        def collect(h):
            if h == 0:
                for m in (1, 2, 3):
                    sq_copy(l, m).wait_recv()
                total = sq_out[inner] + sq_got[0] + sq_got[1] + sq_got[2]
                factor = lax.rsqrt(total * (1.0 / features) + EPS)[0:1]
                scale.append(jnp.transpose(jnp.broadcast_to(factor, (128, rows))))
            for s in range(2, 6):
                rs_copy(h, s).wait_recv()
            for c in range(lanes):
                here = pl.ds(c * pair, pair)
                total = (
                    part[h, inner, :, here].astype(F32)
                    + gotten[h, 0, :, here].astype(F32)
                    + gotten[h, 1, :, here].astype(F32)
                )
                mixed = (total * scale[0]).astype(BF16)
                tail_out[h, :, here] = mixed[rows - 16 :]
                ext[pl.ds(8, rows), here] = mixed.astype(F32)
            tail_copy = send(
                tail_out.at[h], tails.at[l, h], tail_sem.at[l, h, 0], tail_sem.at[l, h, 1],
                sp=after,
            )
            pl.when(not_last)(tail_copy.start)
            tail_copies.append(tail_copy)

        def gates(h):
            pl.when(not_first)(tail_copies[h].wait_recv)
            ext[pl.ds(0, 8), :] = tails[l, h, 8:].astype(F32)

            for c in range(lanes):
                here = pl.ds(c * pair, pair)
                col = h * span + c * pair
                cols = pl.ds(col, pair)
                at = h * lanes + c
                row = slice(l, l + 1)
                conv = bias_ref[row, cols] + taps_ref[l, 0:1, cols] * ext[pl.ds(8, rows), here]
                for lag in range(1, taps):
                    same = docs[pl.ds(8 - lag, rows), :] == docs[pl.ds(8, rows), :]
                    shifted = ext[pl.ds(8 - lag, rows), here]
                    conv = conv + jnp.where(same, taps_ref[l, lag : lag + 1, cols] * shifted, 0.0)
                conv_out = conv.astype(BF16)
                recur = jnp.dot(conv_out, diagonal(rgate_ref, l, col), preferred_element_type=F32)
                inp = jnp.dot(conv_out, diagonal(igate_ref, l, col), preferred_element_type=F32)
                recur = jax.nn.sigmoid(recur + rbias_ref[row, cols])
                inp = jax.nn.sigmoid(inp + ibias_ref[row, cols])
                log_decay = coef[row, cols] * recur
                keep = docs[pl.ds(7, rows), :] == docs[pl.ds(8, rows), :]
                a_buf[at] = jnp.where(keep, jnp.exp(log_decay), 0.0)
                b_buf[at] = jnp.sqrt(jnp.maximum(minus_expm1(2.0 * log_decay), 0.0)) * (
                    inp * conv_out.astype(F32)
                )

            def advance(r, carry):
                at = pl.ds(r, 8, stride=sub)
                following = []
                for c in range(lanes):
                    decay, state = carry[c]
                    a = a_buf[h * lanes + c, at, :]
                    decay = decay * a
                    state = a * state + b_buf[h * lanes + c, at, :]
                    a_buf[h * lanes + c, at, :] = decay
                    b_buf[h * lanes + c, at, :] = state
                    following.append((decay, state))
                return tuple(following)

            start = (jnp.ones((8, pair), F32), jnp.zeros((8, pair), F32))
            chunks = lax.fori_loop(0, sub, advance, (start,) * lanes, unroll=4)
            decay = jnp.concatenate([c[0] for c in chunks], axis=1)
            state = jnp.concatenate([c[1] for c in chunks], axis=1)
            prefix = [(jnp.ones((1, span), F32), jnp.zeros((1, span), F32))]
            for s in range(8):
                d, e = prefix[-1]
                prefix.append((d * decay[s : s + 1], decay[s : s + 1] * e + state[s : s + 1]))
            prefixes.append(prefix)
            ends[l, h, me, 0:1, :] = prefix[8][0]
            ends[l, h, me, 1:2, :] = prefix[8][1]

            def end_to(dst, _):
                pl.when(dst > me)(lambda: end_copy(h, dst, me).start())
                return 0

            lax.fori_loop(0, n_sp, end_to, 0)

        def emit(h):
            def fold(src, state):
                pl.when(src < me)(lambda: end_copy(h, src, src).wait_recv())
                following = ends[l, h, src, 0:1, :] * state + ends[l, h, src, 1:2, :]
                return jnp.where(src < me, following, state)

            carried = lax.fori_loop(0, n_sp, fold, jnp.zeros((1, span), F32))
            for s in range(8):
                at = pl.ds(s * sub, sub)
                enter = prefixes[h][s][0] * carried + prefixes[h][s][1]
                for c in range(lanes):
                    one = enter[:, c * pair : (c + 1) * pair]
                    hid[h, inner, at, pl.ds(c * pair, pair)] = (
                        b_buf[h * lanes + c, at, :] + a_buf[h * lanes + c, at, :] * one
                    ).astype(BF16)
            for s in range(4):
                ag_copy(h, s).start()

        def ag_relay(h):
            ag_arrived(h, 0)
            ag_copy(h, 4).start()
            ag_arrived(h, 1)
            ag_copy(h, 5).start()

        for h in range(halves):
            collect(h)
            if h > 0:
                emit(h - 1)
            gates(h)
            if h > 0:
                ag_relay(h - 1)
            if l == 0:
                weight_relay(0, 1, h)
                if not last:
                    weight_go(1, 0, h)
        emit(halves - 1)
        for q in range(halves):
            weight_wait(l, 1, q)
        ag_relay(halves - 1)

        def tp_copy(j, other, landed):
            peer = lax.rem(core + other, n_tp)
            return send(
                psend.at[j], pgot.at[l, landed, j], tp_send.at[other - 1, j],
                tp_recv.at[l, landed, j], tp=peer,
            )

        def unproject(step, _):
            j = flip(inner, step)
            for s in range(2, 6):
                for h in range(halves):
                    pl.when(step == (1, 2, 3, 3)[s - 2])(functools.partial(ag_arrived, h, s))
            for block in range(outer):
                out = 0.0
                for h in range(halves):
                    out = out + jnp.dot(
                        hid[h, j], wout[l, block, h * span : (h + 1) * span],
                        preferred_element_type=F32,
                    )
                psend[j, :, block * width : (block + 1) * width] = out.astype(BF16)
            for other in range(1, n_tp):
                tp_copy(j, other, n_tp - other - 1).start()
            return 0

        if not last:
            for q in range(halves):
                weight_relay(l + 1, 0, q)
                weight_go(l + 1, 1, q)
        lax.fori_loop(0, g, unproject, 0)

        def f_copy(m, o, src, landed):
            return send(
                slot(xbuf, src, mine, o), piece(o_ref, mine, landed, o), f_send.at[m, o],
                f_recv.at[m, o], sp=member(square, place, flip(inner, m)),
            )

        def finish(step, _):
            j = flip(inner, step)
            for other in range(1, n_tp):
                copy = tp_copy(j, other, other - 1)
                copy.wait_recv()
                copy.wait_send()
            at = mine if last else pl.ds(0, rows)
            summed = psend[j, at, :].astype(F32)
            for other in range(1, n_tp):
                summed = summed + pgot[l, other - 1, j, at, :].astype(F32)
            new = (xbuf[j, at, :].astype(F32) + summed).astype(BF16)
            xbuf[j, at, :] = new
            if last:

                @pl.when(step > 0)
                def _():
                    for o in range(pieces):
                        f_copy(step, o, j, inner).start()

            return 0

        lax.fori_loop(0, g, finish, 0)

        for h in range(halves):
            for s in range(6):
                rs_copy(h, s).wait_send()
                ag_copy(h, s).wait_send()
        for m in (1, 2, 3):
            sq_copy(l, m).wait_send()

        def end_close(dst, _):
            for h in range(halves):
                pl.when(dst > me)(lambda: end_copy(h, dst, me).wait_send())
            return 0

        lax.fori_loop(0, n_sp, end_close, 0)
        for tail_copy in tail_copies:
            pl.when(not_last)(tail_copy.wait_send)
        if not last:
            for q in range(halves):
                weight_relay(l + 1, 1, q)

    for o in range(pieces):
        target = piece(o_ref, mine, inner, o)
        target[...] = slot(xbuf, inner, mine, o)[...]

    def f_arrive(m, _):
        j = flip(inner, m)
        for o in range(pieces):
            f_copy(m, o, j, j).wait_recv()
        return 0

    lax.fori_loop(1, g, f_arrive, 0)

    def share_of(at):
        return o_ref.at[at] if strided else o_ref.at[:, at]

    def f_share(other, at, landed):
        return send(
            share_of(at), share_of(at), ft_send.at[other - 1], ft_recv.at[landed],
            tp=lax.rem(core + other, n_tp),
        )

    for other in range(1, n_tp):
        f_share(other, mine, n_tp - other - 1).start()
    for l in range(layers):
        for kind in range(2):
            for q in range(halves):
                weight_close(l, kind, q)

    def f_close(m, _):
        j = flip(inner, m)
        for o in range(pieces):
            f_copy(m, o, j, inner).wait_send()
        return 0

    lax.fori_loop(1, g, f_close, 0)
    for other in range(1, n_tp):
        peer = lax.rem(core + other, n_tp)
        f_share(other, pl.ds(peer * half, half), other - 1).wait_recv()
        f_share(other, mine, other - 1).wait_send()


def per_device(
    tokens,
    documents,
    norm_gain,
    in_weight,
    conv_taps,
    conv_bias,
    recur_gate,
    input_gate,
    recur_bias,
    input_bias,
    decay_param,
    out_weight,
):
    g = G
    n_sp, n_tp = lax.axis_size("sp"), lax.axis_size("tp")
    outer = n_sp // g
    rows, features = tokens.shape
    layers, width, chans = in_weight.shape
    strided = width % 128 == 0
    square = strided and n_sp == 16
    pieces = outer if strided else 1
    part_width = outer * width
    halves = 2 if chans % 256 == 0 else 1
    span = chans // halves
    x, gain = tokens, norm_gain
    if not strided:
        inner = lax.rem(lax.axis_index("sp"), g)
        x = x.reshape(rows, outer, g, width).transpose(2, 0, 1, 3).reshape(g, rows, part_width)
        gain = norm_gain.reshape(layers, outer, g, width)
        gain = lax.dynamic_index_in_dim(gain, inner, 2, False).reshape(layers, part_width)
    dim = recur_gate.shape[2]
    slots = max(outer, 3)
    dma = pltpu.SemaphoreType.DMA
    any_space = pl.BlockSpec(memory_space=pl.ANY)
    others = max(n_tp - 1, 1)
    out = pl.pallas_call(
        functools.partial(whole_kernel, n_sp, n_tp, square),
        out_shape=jax.ShapeDtypeStruct(x.shape, x.dtype),
        in_specs=[any_space] * 3 + [VM] * 9,
        out_specs=VM,
        scratch_shapes=[
            pltpu.VMEM((g, rows, part_width), BF16),
            pltpu.VMEM((layers, part_width, chans), BF16),
            pltpu.VMEM((layers, outer, chans, width), BF16),
            pltpu.VMEM((halves, g, rows, span), BF16),
            pltpu.VMEM((halves, 3, rows, span), BF16),
            pltpu.VMEM((g, 8, rows), F32),
            pltpu.VMEM((3, 8, rows), F32),
            pltpu.VMEM((layers, halves, 16, span), BF16),
            pltpu.VMEM((halves, 16, span), BF16),
            pltpu.VMEM((8, 128), F32),
            pltpu.VMEM((rows + 8, 128), F32),
            pltpu.VMEM((layers, part_width), F32),
            pltpu.VMEM((layers, chans), F32),
            pltpu.VMEM((rows + 8, span), F32),
            pltpu.VMEM((chans // 128, rows, 128), F32),
            pltpu.VMEM((chans // 128, rows, 128), F32),
            pltpu.VMEM((layers, halves, n_sp, 2, span), F32),
            pltpu.VMEM((halves, g, rows, span), BF16),
            pltpu.VMEM((g, rows, part_width), BF16),
            pltpu.VMEM((layers, others, g, rows, part_width), BF16),
            dma((2 * layers, halves)),
            dma((pieces,)),
            dma((g, pieces)),
            dma((g, pieces)),
            dma((g, others)),
            dma((g, others)),
            dma((2 * layers, halves, slots)),
            dma((2 * layers, halves, slots)),
            dma((2,)),
            dma((halves, 6)),
            dma((halves, 6)),
            dma((3,)),
            dma((3,)),
            dma((layers, halves, 2)),
            dma((layers, halves, n_sp)),
            dma((layers, halves, n_sp)),
            dma((halves, 6)),
            dma((halves, 6)),
            dma((others, g)),
            dma((layers, others, g)),
            dma((g, pieces)),
            dma((g, pieces)),
            dma((others,)),
            dma((others,)),
        ],
        compiler_params=pltpu.CompilerParams(
            has_side_effects=True, vmem_limit_bytes=60 * 1024 * 1024
        ),
    )(
        x, in_weight, out_weight, documents.reshape(1, rows), gain, conv_taps, conv_bias,
        recur_bias, input_bias, decay_param,
        recur_gate.reshape(layers, chans, dim), input_gate.reshape(layers, chans, dim),
    )
    if not strided:
        out = out.reshape(g, rows, outer, width).transpose(1, 2, 0, 3).reshape(rows, features)
    return out


def solution(mesh):
    return jax.shard_map(
        per_device,
        mesh=mesh,
        in_specs=(
            P("sp", None),
            P("sp"),
            P(),
            P(None, "sp", "tp"),
            P(None, None, "tp"),
            P(None, "tp"),
            P(None, "tp", None, None),
            P(None, "tp", None, None),
            P(None, "tp"),
            P(None, "tp"),
            P(None, "tp"),
            P(None, "tp", "sp"),
        ),
        out_specs=P("sp", None),
        check_vma=False,
    )
```

```python
import functools

import jax
import jax.numpy as jnp
from jax import lax
from jax.experimental import pallas as pl
from jax.experimental.pallas import tpu as pltpu
from jax.sharding import PartitionSpec as P

RG_C = 8.0
EPS = 0.1
G = 4
FIRST_WAY = (3 / 4, 5 / 8)
TAIL = 16
MESH = pl.DeviceIdType.MESH
F32 = jnp.float32
BF16 = jnp.bfloat16
VM = pl.BlockSpec(memory_space=pltpu.VMEM)


def send(src, dst, send_sem, recv_sem, **device):
    return pltpu.make_async_remote_copy(
        src_ref=src,
        dst_ref=dst,
        send_sem=send_sem,
        recv_sem=recv_sem,
        device_id=device,
        device_id_type=MESH,
    )


def minus_expm1(x):
    series = 1.0 + x * (1.0 / 8.0)
    for n in range(7, 1, -1):
        series = 1.0 + (x * (1.0 / n)) * series
    return jnp.where(x > -0.5, -x * series, 1.0 - jnp.exp(x))


def flip(i, m):
    return 2 * lax.rem(i // 2 + m // 2, 2) + lax.rem(i + m, 2)


def member(square, o, j):
    if square:
        return (o // 2) * 8 + (j // 2) * 4 + (o % 2) * 2 + j % 2
    return o * G + j


def whole_kernel(
    n_sp, n_tp, square,
    x_in, win_in, wout_in, doc_ref, gain_ref, taps_ref, bias_ref, rbias_ref, ibias_ref, decay_ref,
    rgate_ref, igate_ref,
    o_ref,
    xbuf, win, wout, part, gotten, sq_out, sq_got, tip_in, tip_out, tip_got, tails, tail_out, doc_tail, docs, gain, coef,
    ext, a_buf, b_buf, ends, hid, psend, pgot,
    own_sem, x_own, x_send, x_recv, xt_send, xt_recv, w_send, w_recv, doc_sem, rs_send, rs_recv,
    sq_send, sq_recv, tip_send, tip_recv, tail_sem, end_send, end_recv, ag_send, ag_recv, tp_send, tp_recv, f_send,
    f_recv, ft_send, ft_recv,
):
    g = G
    me = lax.axis_index("sp")
    core = lax.axis_index("tp")
    outer = n_sp // g
    if square:
        inner = 2 * lax.rem(me // 4, 2) + lax.rem(me, 2)
        place = 2 * (me // 8) + lax.rem(me // 2, 2)
    else:
        inner, place = lax.rem(me, g), me // g
    near = {m: flip(inner, m) for m in (1, 2, 3)}
    at_sp = {m: member(square, place, near[m]) for m in (1, 2, 3)}
    layers, width, chans = win_in.shape
    rows, features = xbuf.shape[1], xbuf.shape[2] * g
    taps = taps_ref.shape[1]
    halves, span = hid.shape[0], hid.shape[3]
    half = rows // n_tp
    mine = pl.ds(core * half, half)
    strided = len(x_in.shape) == 2
    pieces = outer if strided else 1
    after = lax.rem(me + 1, n_sp)
    not_last, not_first = me < n_sp - 1, me > 0

    def ways(l):
        cut = int(rows * FIRST_WAY[min(l, 1)]) // 16 * 16
        return pl.ds(0, cut), pl.ds(cut, rows - cut)

    def piece(ref, at, j, o):
        if strided:
            return ref.at[at, pl.ds(pl.multiple_of(member(square, o, j) * width, width), width)]
        return ref.at[j, at, :]

    def slot(ref, j, at, o):
        return ref.at[j, at, pl.ds(o * width, width)] if strided else ref.at[j, at, :]

    def wref(l, kind, q):
        if kind == 0:
            return win_in.at[l, :, pl.ds(q * span, span)]
        return wout_in.at[l, pl.ds(q * span, span), :]

    def wslot(l, kind, q, o):
        if kind == 0:
            return win.at[l, pl.ds(o * width, width), pl.ds(q * span, span)]
        return wout.at[l, o, pl.ds(q * span, span), :]

    def weight_own(l, kind, q):
        return pltpu.make_async_copy(
            wref(l, kind, q), wslot(l, kind, q, place), own_sem.at[2 * l + kind, q]
        )

    def weight_copy(l, kind, q, to, src, o, sem, landed):
        k = 2 * l + kind
        return send(
            src, wslot(l, kind, q, o), w_send.at[k, q, sem], w_recv.at[k, q, landed],
            sp=member(square, to, inner),
        )

    def weight_copies(l, kind, q):
        own = wref(l, kind, q)
        if square:
            return [
                weight_copy(l, kind, q, flip(place, m), own, place, s, s)
                for s, m in enumerate((2, 1))
            ]
        copies = []
        for step in range(1, outer):
            to = lax.rem(place + step, outer)
            copies.append(weight_copy(l, kind, q, to, own, place, to, place))
        return copies

    def weight_go(l, kind, q, which=None):
        if q < halves and l < layers:
            copies = weight_copies(l, kind, q)
            for copy in copies if which is None or not square else copies[which : which + 1]:
                copy.start()

    def weight_forward(l, kind, q):
        o = flip(place, 2)
        return weight_copy(l, kind, q, flip(place, 1), wslot(l, kind, q, o), o, 2, 2)

    def weight_arrived(l, kind, q, o, sem):
        weight_copy(l, kind, q, flip(place, 1), wslot(l, kind, q, o), o, 0, sem).wait_recv()

    def weight_relay(l, kind, q):
        if square and q < halves and l < layers:
            weight_arrived(l, kind, q, flip(place, 2), 0)
            weight_forward(l, kind, q).start()

    def weight_wait(l, kind, q):
        weight_own(l, kind, q).wait()
        if square:
            weight_arrived(l, kind, q, flip(place, 1), 1)
            weight_arrived(l, kind, q, flip(place, 3), 2)
        else:
            for step in range(1, outer):
                o = lax.rem(place + step, outer)
                src = wref(l, kind, q)
                weight_copy(l, kind, q, o, src, o, o, o).wait_recv()

    def weight_close(l, kind, q):
        for copy in weight_copies(l, kind, q):
            copy.wait_send()
        if square:
            weight_forward(l, kind, q).wait_send()

    def x_copy(m, o, landed):
        j = flip(inner, m)
        return send(
            piece(x_in, mine, j, o),
            slot(xbuf, landed, mine, o),
            x_send.at[m, o],
            x_recv.at[m, o],
            sp=member(square, place, j),
        )

    def own_piece(o):
        everything = pl.ds(0, rows)
        return pltpu.make_async_copy(
            piece(x_in, everything, inner, o), slot(xbuf, inner, everything, o), x_own.at[o]
        )

    weight_go(0, 0, 0)

    def x_go(step, _):
        for o in range(pieces):
            x_copy(g - step, o, inner).start()
        return 0

    lax.fori_loop(1, g, x_go, 0)
    if square:
        weight_go(0, 0, 1, 1)
    for o in range(pieces):
        own_piece(o).start()
    for l in range(layers):
        for kind in range(2):
            for q in range(halves):
                weight_own(l, kind, q).start()

    column = jnp.broadcast_to(doc_ref[...].astype(F32), (128, rows))
    docs[pl.ds(8, rows), :] = jnp.transpose(column)
    doc_copy = send(
        docs.at[pl.ds(rows, 8)], doc_tail, doc_sem.at[0], doc_sem.at[1], sp=after
    )
    pl.when(not_last)(doc_copy.start)

    @pl.when(me == 0)
    def _():
        doc_tail[...] = jnp.full(doc_tail.shape, -1.0, F32)
        tails[...] = jnp.zeros(tails.shape, BF16)

    coef[...] = -RG_C * jax.nn.softplus(-decay_ref[...])
    if strided:
        for o in range(outer):
            at = pl.ds(pl.multiple_of(member(square, o, inner) * width, width), width)
            gain[:, pl.ds(o * width, width)] = gain_ref[:, at]
    else:
        gain[...] = gain_ref[...]

    def x_share(j, other, at):
        peer = lax.rem(core + other, n_tp)
        return send(
            xbuf.at[j, at], xbuf.at[j, at], xt_send.at[j, other - 1],
            xt_recv.at[j, n_tp - other - 1], tp=peer,
        )

    def x_arrive(m, _):
        j = flip(inner, m)
        for o in range(pieces):
            x_copy(m, o, j).wait_recv()
        for other in range(1, n_tp):
            x_share(j, other, mine).start()
        return 0

    weight_relay(0, 0, 0)
    weight_go(0, 0, 1, 0)
    lax.fori_loop(1, g, x_arrive, 0)
    for o in range(pieces):
        own_piece(o).wait()

    pl.when(not_first)(doc_copy.wait_recv)
    docs[pl.ds(0, 8), :] = doc_tail[...]

    def x_shared(m, _):
        j = flip(inner, m)
        for other in range(1, n_tp):
            peer = lax.rem(core + other, n_tp)
            at = pl.ds(peer * half, half)
            send(
                xbuf.at[j, at], xbuf.at[j, at], xt_send.at[j, other - 1],
                xt_recv.at[j, other - 1], tp=peer,
            ).wait_recv()
            x_share(j, other, mine).wait_send()
        for o in range(pieces):
            x_copy(m, o, inner).wait_send()
        return 0

    lax.fori_loop(1, g, x_shared, 0)
    pl.when(not_last)(doc_copy.wait_send)

    pair = 128
    dim = rgate_ref.shape[2]
    repeat = (
        lax.rem(lax.broadcasted_iota(jnp.int32, (dim, pair), 1), dim)
        == lax.broadcasted_iota(jnp.int32, (dim, pair), 0)
    ).astype(F32).astype(BF16)
    on_block = (
        lax.broadcasted_iota(jnp.int32, (pair, pair), 0) // dim
        == lax.broadcasted_iota(jnp.int32, (pair, pair), 1) // dim
    )

    def diagonal(ref, l, col):
        wide = jnp.dot(ref[l, pl.ds(col, pair), :], repeat, preferred_element_type=F32)
        return jnp.where(on_block, wide, 0.0).astype(BF16)

    sub = rows // 8
    lanes = span // pair

    def rs_copy(l, h, s):
        r0, r1 = ways(l)
        j, at, lands, to = (
            (3, r0, 2, 1), (3, r1, 2, 2), (1, r0, 0, 1), (2, r1, 1, 2), (2, r0, 1, 2),
            (1, r1, 0, 1),
        )[s]
        return send(
            part.at[h, near[j], at], gotten.at[h, lands, at], rs_send.at[h, s],
            rs_recv.at[h, s], sp=at_sp[to],
        )

    def ag_copy(l, h, s):
        r0, r1 = ways(l)
        j, at, to = (
            (0, r0, 1), (0, r1, 2), (0, r1, 1), (0, r0, 2), (1, r0, 2), (2, r1, 1),
        )[s]
        ref = hid.at[h, near[j] if j else inner, at]
        return send(ref, ref, ag_send.at[h, s], ag_recv.at[h, s], sp=at_sp[to])

    def ag_arrived(l, h, s):
        r0, r1 = ways(l)
        j, at = ((1, r0), (2, r1), (1, r1), (2, r0), (3, r0), (3, r1))[s]
        ref = hid.at[h, near[j], at]
        send(ref, ref, ag_send.at[h, s], ag_recv.at[h, s], sp=at_sp[1]).wait_recv()

    def f_copy(m, o, src, landed):
        return send(
            slot(xbuf, src, mine, o), piece(o_ref, mine, landed, o), f_send.at[m, o],
            f_recv.at[m, o], sp=member(square, place, flip(inner, m)),
        )

    def sq_copy(l, m):
        return send(
            sq_out.at[near[m]], sq_got.at[m - 1], sq_send.at[m - 1], sq_recv.at[m - 1],
            sp=at_sp[m],
        )

    def tip_copy(h, m):
        return send(
            tip_out.at[h, near[m]], tip_got.at[h, m - 1], tip_send.at[h, m - 1],
            tip_recv.at[h, m - 1], sp=at_sp[m],
        )

    def ag_close(l):
        for h in range(halves):
            for s in range(6):
                ag_copy(l, h, s).wait_send()

    tail_copies = [[] for _ in range(layers)]
    for l in range(layers):
        last = l == layers - 1

        r0, r1 = ways(l)

        def rs_relay(h):
            rs_copy(l, h, 0).wait_recv()
            part[h, near[2], r0] = (
                part[h, near[2], r0].astype(F32) + gotten[h, 2, r0].astype(F32)
            ).astype(BF16)
            rs_copy(l, h, 4).start()
            rs_copy(l, h, 1).wait_recv()
            part[h, near[1], r1] = (
                part[h, near[1], r1].astype(F32) + gotten[h, 2, r1].astype(F32)
            ).astype(BF16)
            rs_copy(l, h, 5).start()

        def prepare(step, _):
            m = jnp.where(step < 2, 3 - 2 * step, 6 - 2 * step)
            j = flip(inner, m)
            x = xbuf[j].astype(F32)
            squares = jnp.sum(x * x, axis=1, keepdims=True)
            sq_out[j] = jnp.transpose(jnp.broadcast_to(squares, (rows, 128)))[0:8]
            for n in (1, 2, 3):
                pl.when(m == n)(sq_copy(l, n).start)
            normed = (x * gain[l : l + 1, :]).astype(BF16)
            psend[j] = normed
            tip_in[j] = normed[rows - TAIL :]
            return 0

        lax.fori_loop(0, g, prepare, 0)
        scale = []
        prefixes = []

        def tail(h):
            if h == 0:
                for m in (1, 2, 3):
                    sq_copy(l, m).wait_recv()
                total = sq_out[inner] + sq_got[0] + sq_got[1] + sq_got[2]
                factor = lax.rsqrt(total * (1.0 / features) + EPS)[0:1]
                scale.append(jnp.transpose(jnp.broadcast_to(factor, (128, rows))))
            for m in (1, 2, 3):
                tip_copy(h, m).wait_recv()
            for c in range(lanes):
                here = pl.ds(c * pair, pair)
                total = tip_out[h, inner, :, here].astype(F32)
                for m in range(3):
                    total = total + tip_got[h, m, :, here].astype(F32)
                tail_out[l, h, :, here] = (total * scale[0][rows - TAIL :]).astype(BF16)
            tail_copy = send(
                tail_out.at[l, h], tails.at[l, h], tail_sem.at[l, h, 0], tail_sem.at[l, h, 1],
                sp=after,
            )
            pl.when(not_last)(tail_copy.start)
            tail_copies[l].append(tail_copy)

        for h in range(halves):
            weight_wait(l, 0, h)
            tips = tip_in[...].reshape(g * TAIL, -1)
            tips = jnp.dot(
                tips, win[l, :, h * span : (h + 1) * span], preferred_element_type=F32
            )
            tip_out[h] = tips.astype(BF16).reshape(g, TAIL, span)
            for m in (1, 2, 3):
                tip_copy(h, m).start()

            def project(step, _):
                m = jnp.where(step < 2, 3 - 2 * step, 6 - 2 * step)
                j = flip(inner, m)
                out = jnp.dot(
                    psend[j], win[l, :, h * span : (h + 1) * span], preferred_element_type=F32
                )
                part[h, j] = out.astype(BF16)

                @pl.when(step == 0)
                def _():
                    rs_copy(l, h, 0).start()
                    rs_copy(l, h, 1).start()

                pl.when(step == 1)(rs_copy(l, h, 2).start)
                pl.when(step == 2)(rs_copy(l, h, 3).start)
                return 0

            lax.fori_loop(0, g, project, 0)
            tail(h)
            if h == 0:
                weight_relay(l, 0, 1)
                weight_go(l, 1, 0)
                if l > 0:
                    ag_close(l - 1)
                rs_relay(0)
        weight_go(l, 1, 1)

        def end_copy(h, dst, src, l=l):
            return send(
                ends.at[l, h, me], ends.at[l, h, src], end_send.at[l, h, dst],
                end_recv.at[l, h, src], sp=dst,
            )

        def collect(h):
            for s in range(2, 6):
                rs_copy(l, h, s).wait_recv()
            for c in range(lanes):
                here = pl.ds(c * pair, pair)
                total = (
                    part[h, inner, :, here].astype(F32)
                    + gotten[h, 0, :, here].astype(F32)
                    + gotten[h, 1, :, here].astype(F32)
                )
                mixed = (total * scale[0]).astype(BF16)
                ext[pl.ds(8, rows), here] = mixed.astype(F32)

        def gates(h):
            pl.when(not_first)(tail_copies[l][h].wait_recv)
            ext[pl.ds(0, 8), :] = tails[l, h, TAIL - 8 :].astype(F32)

            for c in range(lanes):
                here = pl.ds(c * pair, pair)
                col = h * span + c * pair
                cols = pl.ds(col, pair)
                at = h * lanes + c
                row = slice(l, l + 1)
                conv = bias_ref[row, cols] + taps_ref[l, 0:1, cols] * ext[pl.ds(8, rows), here]
                for lag in range(1, taps):
                    same = docs[pl.ds(8 - lag, rows), :] == docs[pl.ds(8, rows), :]
                    shifted = ext[pl.ds(8 - lag, rows), here]
                    conv = conv + jnp.where(same, taps_ref[l, lag : lag + 1, cols] * shifted, 0.0)
                conv_out = conv.astype(BF16)
                recur = jnp.dot(conv_out, diagonal(rgate_ref, l, col), preferred_element_type=F32)
                inp = jnp.dot(conv_out, diagonal(igate_ref, l, col), preferred_element_type=F32)
                recur = jax.nn.sigmoid(recur + rbias_ref[row, cols])
                inp = jax.nn.sigmoid(inp + ibias_ref[row, cols])
                log_decay = coef[row, cols] * recur
                keep = docs[pl.ds(7, rows), :] == docs[pl.ds(8, rows), :]
                a_buf[at] = jnp.where(keep, jnp.exp(log_decay), 0.0)
                b_buf[at] = jnp.sqrt(jnp.maximum(minus_expm1(2.0 * log_decay), 0.0)) * (
                    inp * conv_out.astype(F32)
                )

            def advance(r, carry):
                at = pl.ds(r, 8, stride=sub)
                following = []
                for c in range(lanes):
                    decay, state = carry[c]
                    a = a_buf[h * lanes + c, at, :]
                    decay = decay * a
                    state = a * state + b_buf[h * lanes + c, at, :]
                    a_buf[h * lanes + c, at, :] = decay
                    b_buf[h * lanes + c, at, :] = state
                    following.append((decay, state))
                return tuple(following)

            start = (jnp.ones((8, pair), F32), jnp.zeros((8, pair), F32))
            chunks = lax.fori_loop(0, sub, advance, (start,) * lanes, unroll=4)
            decay = jnp.concatenate([c[0] for c in chunks], axis=1)
            state = jnp.concatenate([c[1] for c in chunks], axis=1)
            prefix = [(jnp.ones((1, span), F32), jnp.zeros((1, span), F32))]
            for s in range(8):
                d, e = prefix[-1]
                prefix.append((d * decay[s : s + 1], decay[s : s + 1] * e + state[s : s + 1]))
            prefixes.append(prefix)
            ends[l, h, me, 0:1, :] = prefix[8][0]
            ends[l, h, me, 1:2, :] = prefix[8][1]

            def end_to(dst, _):
                pl.when(dst > me)(lambda: end_copy(h, dst, me).start())
                return 0

            lax.fori_loop(0, n_sp, end_to, 0)

        def emit(h):
            def fold(src, state):
                pl.when(src < me)(lambda: end_copy(h, src, src).wait_recv())
                following = ends[l, h, src, 0:1, :] * state + ends[l, h, src, 1:2, :]
                return jnp.where(src < me, following, state)

            carried = lax.fori_loop(0, n_sp, fold, jnp.zeros((1, span), F32))
            for s in range(8):
                at = pl.ds(s * sub, sub)
                enter = prefixes[h][s][0] * carried + prefixes[h][s][1]
                for c in range(lanes):
                    one = enter[:, c * pair : (c + 1) * pair]
                    hid[h, inner, at, pl.ds(c * pair, pair)] = (
                        b_buf[h * lanes + c, at, :] + a_buf[h * lanes + c, at, :] * one
                    ).astype(BF16)
            for s in range(4):
                ag_copy(l, h, s).start()

        def ag_relay(h):
            ag_arrived(l, h, 0)
            ag_copy(l, h, 4).start()
            ag_arrived(l, h, 1)
            ag_copy(l, h, 5).start()

        for h in range(halves):
            collect(h)
            if h == halves - 1:
                weight_relay(l, 1, 1)
            if h > 0:
                emit(h - 1)
            gates(h)
            if h == 0:
                weight_relay(l, 1, 0)
            if h + 1 < halves:
                rs_relay(h + 1)
            else:
                weight_go(l + 1, 0, 0)
                weight_go(l + 1, 0, 1)
            if h > 0:
                ag_relay(h - 1)
        emit(halves - 1)
        for q in range(halves):
            weight_wait(l, 1, q)
        ag_relay(halves - 1)

        def tp_copy(j, other, landed):
            peer = lax.rem(core + other, n_tp)
            return send(
                psend.at[j], pgot.at[l, landed, j], tp_send.at[other - 1, j],
                tp_recv.at[l, landed, j], tp=peer,
            )

        def unproject(step):
            j = flip(inner, step)
            for s in range(2, 6):
                for h in range(halves):
                    pl.when(step == (1, 2, 3, 3)[s - 2])(functools.partial(ag_arrived, l, h, s))
            for block in range(outer):
                out = 0.0
                for h in range(halves):
                    out = out + jnp.dot(
                        hid[h, j], wout[l, block, h * span : (h + 1) * span],
                        preferred_element_type=F32,
                    )
                psend[j, :, block * width : (block + 1) * width] = out.astype(BF16)
            for other in range(1, n_tp):
                tp_copy(j, other, n_tp - other - 1).start()

        def finish(step):
            j = flip(inner, step)
            for other in range(1, n_tp):
                copy = tp_copy(j, other, other - 1)
                copy.wait_recv()
                copy.wait_send()
            at = mine if last else pl.ds(0, rows)
            summed = psend[j, at, :].astype(F32)
            for other in range(1, n_tp):
                summed = summed + pgot[l, other - 1, j, at, :].astype(F32)
            new = (xbuf[j, at, :].astype(F32) + summed).astype(BF16)
            xbuf[j, at, :] = new
            if last:

                @pl.when(step > 0)
                def _():
                    for o in range(pieces):
                        f_copy(step, o, j, inner).start()

        def both(step, _):
            pl.when(step < g)(lambda: unproject(step))
            pl.when(step > 0)(lambda: finish(step - 1))
            if square:
                if not last:
                    pl.when(step == 1)(lambda: weight_relay(l + 1, 0, 0))
            return 0

        lax.fori_loop(0, g + 1, both, 0)

        for h in range(halves):
            for s in range(6):
                rs_copy(l, h, s).wait_send()
        for m in (1, 2, 3):
            sq_copy(l, m).wait_send()
            for h in range(halves):
                tip_copy(h, m).wait_send()

    def f_share(j, o, other, at, landed):
        ref = piece(o_ref, at, j, o)
        return send(
            ref, ref, ft_send.at[other - 1, j, o], ft_recv.at[landed, j, o],
            tp=lax.rem(core + other, n_tp),
        )

    def f_arrive(m, _):
        j = flip(inner, m)
        for o in range(pieces):
            pl.when(m > 0)(lambda: f_copy(m, o, j, j).wait_recv())
            for other in range(1, n_tp):
                f_share(j, o, other, mine, n_tp - other - 1).start()
        return 0

    for o in range(pieces):
        target = piece(o_ref, mine, inner, o)
        target[...] = slot(xbuf, inner, mine, o)[...]
    lax.fori_loop(0, g, f_arrive, 0)

    ag_close(layers - 1)
    for l in range(layers):
        for kind in range(2):
            for q in range(halves):
                weight_close(l, kind, q)
        for tail_copy in tail_copies[l]:
            pl.when(not_last)(tail_copy.wait_send)

    def end_close(dst, _):
        @pl.when(dst > me)
        def _():
            for l in range(layers):
                for h in range(halves):
                    ref = ends.at[l, h, me]
                    send(
                        ref, ref, end_send.at[l, h, dst], end_recv.at[l, h, me], sp=dst
                    ).wait_send()

        return 0

    lax.fori_loop(0, n_sp, end_close, 0)

    def f_close(m, _):
        j = flip(inner, m)
        for o in range(pieces):
            pl.when(m > 0)(lambda: f_copy(m, o, j, inner).wait_send())
            for other in range(1, n_tp):
                peer = lax.rem(core + other, n_tp)
                f_share(j, o, other, pl.ds(peer * half, half), other - 1).wait_recv()
                f_share(j, o, other, mine, other - 1).wait_send()
        return 0

    lax.fori_loop(0, g, f_close, 0)


def per_device(
    tokens,
    documents,
    norm_gain,
    in_weight,
    conv_taps,
    conv_bias,
    recur_gate,
    input_gate,
    recur_bias,
    input_bias,
    decay_param,
    out_weight,
):
    g = G
    n_sp, n_tp = lax.axis_size("sp"), lax.axis_size("tp")
    outer = n_sp // g
    rows, features = tokens.shape
    layers, width, chans = in_weight.shape
    strided = width % 128 == 0
    square = strided and n_sp == 16
    pieces = outer if strided else 1
    part_width = outer * width
    halves = 2 if chans % 256 == 0 else 1
    span = chans // halves
    x, gain = tokens, norm_gain
    if not strided:
        inner = lax.rem(lax.axis_index("sp"), g)
        x = x.reshape(rows, outer, g, width).transpose(2, 0, 1, 3).reshape(g, rows, part_width)
        gain = norm_gain.reshape(layers, outer, g, width)
        gain = lax.dynamic_index_in_dim(gain, inner, 2, False).reshape(layers, part_width)
    dim = recur_gate.shape[2]
    slots = max(outer, 3)
    dma = pltpu.SemaphoreType.DMA
    any_space = pl.BlockSpec(memory_space=pl.ANY)
    others = max(n_tp - 1, 1)
    out = pl.pallas_call(
        functools.partial(whole_kernel, n_sp, n_tp, square),
        out_shape=jax.ShapeDtypeStruct(x.shape, x.dtype),
        in_specs=[any_space] * 3 + [VM] * 9,
        out_specs=VM,
        scratch_shapes=[
            pltpu.VMEM((g, rows, part_width), BF16),
            pltpu.VMEM((layers, part_width, chans), BF16),
            pltpu.VMEM((layers, outer, chans, width), BF16),
            pltpu.VMEM((halves, g, rows, span), BF16),
            pltpu.VMEM((halves, 3, rows, span), BF16),
            pltpu.VMEM((g, 8, rows), F32),
            pltpu.VMEM((3, 8, rows), F32),
            pltpu.VMEM((g, TAIL, part_width), BF16),
            pltpu.VMEM((halves, g, TAIL, span), BF16),
            pltpu.VMEM((halves, 3, TAIL, span), BF16),
            pltpu.VMEM((layers, halves, TAIL, span), BF16),
            pltpu.VMEM((layers, halves, TAIL, span), BF16),
            pltpu.VMEM((8, 128), F32),
            pltpu.VMEM((rows + 8, 128), F32),
            pltpu.VMEM((layers, part_width), F32),
            pltpu.VMEM((layers, chans), F32),
            pltpu.VMEM((rows + 8, span), F32),
            pltpu.VMEM((chans // 128, rows, 128), F32),
            pltpu.VMEM((chans // 128, rows, 128), F32),
            pltpu.VMEM((layers, halves, n_sp, 2, span), F32),
            pltpu.VMEM((halves, g, rows, span), BF16),
            pltpu.VMEM((g, rows, part_width), BF16),
            pltpu.VMEM((layers, others, g, rows, part_width), BF16),
            dma((2 * layers, halves)),
            dma((pieces,)),
            dma((g, pieces)),
            dma((g, pieces)),
            dma((g, others)),
            dma((g, others)),
            dma((2 * layers, halves, slots)),
            dma((2 * layers, halves, slots)),
            dma((2,)),
            dma((halves, 6)),
            dma((halves, 6)),
            dma((3,)),
            dma((3,)),
            dma((halves, 3)),
            dma((halves, 3)),
            dma((layers, halves, 2)),
            dma((layers, halves, n_sp)),
            dma((layers, halves, n_sp)),
            dma((halves, 6)),
            dma((halves, 6)),
            dma((others, g)),
            dma((layers, others, g)),
            dma((g, pieces)),
            dma((g, pieces)),
            dma((others, g, pieces)),
            dma((others, g, pieces)),
        ],
        compiler_params=pltpu.CompilerParams(
            has_side_effects=True, vmem_limit_bytes=60 * 1024 * 1024
        ),
    )(
        x, in_weight, out_weight, documents.reshape(1, rows), gain, conv_taps, conv_bias,
        recur_bias, input_bias, decay_param,
        recur_gate.reshape(layers, chans, dim), input_gate.reshape(layers, chans, dim),
    )
    if not strided:
        out = out.reshape(g, rows, outer, width).transpose(1, 2, 0, 3).reshape(rows, features)
    return out


def solution(mesh):
    return jax.shard_map(
        per_device,
        mesh=mesh,
        in_specs=(
            P("sp", None),
            P("sp"),
            P(),
            P(None, "sp", "tp"),
            P(None, None, "tp"),
            P(None, "tp"),
            P(None, "tp", None, None),
            P(None, "tp", None, None),
            P(None, "tp"),
            P(None, "tp"),
            P(None, "tp"),
            P(None, "tp", "sp"),
        ),
        out_specs=P("sp", None),
        check_vma=False,
    )
```

```python
import functools

import jax
import jax.numpy as jnp
from jax import lax
from jax.experimental import pallas as pl
from jax.experimental.pallas import tpu as pltpu
from jax.sharding import PartitionSpec as P

RG_C = 8.0
EPS = 0.1
G = 4
SUM_WAY = (3 / 4, 5 / 8)
GATHER_WAY = (1 / 4, 3 / 8)
TAIL = 16
PLAN = (
    (
        (0, "relay", 0, 0, 3), (0, "go", 0, 1, 0), (0, "go", 0, 1, 1), (2, "go", 0, 1, 2),
        (2, "go", 0, 1, 3), (3, "relay", 0, 1, 0), (3, "relay", 0, 1, 1), (8, "relay", 0, 1, 2),
        (8, "relay", 0, 1, 3), (5, "go", 1, 0, 0), (9, "go", 1, 0, 1), (9, "go", 1, 0, 2),
        (9, "go", 1, 0, 3), (9, "relay", 1, 0, 0), (10, "relay", 1, 0, 1), (11, "relay", 1, 0, 2),
    ),
    (
        (0, "relay", 0, 0, 3), (0, "go", 0, 1, 0), (0, "go", 0, 1, 1), (2, "go", 0, 1, 2),
        (2, "go", 0, 1, 3), (3, "relay", 0, 1, 0), (3, "relay", 0, 1, 1), (8, "relay", 0, 1, 2),
        (8, "relay", 0, 1, 3),
    ),
)
MESH = pl.DeviceIdType.MESH
F32 = jnp.float32
BF16 = jnp.bfloat16
VM = pl.BlockSpec(memory_space=pltpu.VMEM)


def send(src, dst, send_sem, recv_sem, **device):
    return pltpu.make_async_remote_copy(
        src_ref=src,
        dst_ref=dst,
        send_sem=send_sem,
        recv_sem=recv_sem,
        device_id=device,
        device_id_type=MESH,
    )


def minus_expm1(x):
    series = 1.0 + x * (1.0 / 8.0)
    for n in range(7, 1, -1):
        series = 1.0 + (x * (1.0 / n)) * series
    return jnp.where(x > -0.5, -x * series, 1.0 - jnp.exp(x))


def flip(i, m):
    return 2 * lax.rem(i // 2 + m // 2, 2) + lax.rem(i + m, 2)


def member(square, o, j):
    if square:
        return (o // 2) * 8 + (j // 2) * 4 + (o % 2) * 2 + j % 2
    return o * G + j


def whole_kernel(
    n_sp, n_tp, square,
    x_in, win_in, wout_in, doc_ref, gain_ref, taps_ref, bias_ref, rbias_ref, ibias_ref, decay_ref,
    rgate_ref, igate_ref,
    o_ref,
    xbuf, win, wout, part, gotten, sq_out, sq_got, tip_in, tip_out, tip_got, tails, tail_out, doc_tail, docs, gain, coef,
    ext, a_buf, b_buf, ends, hid, psend, pgot,
    own_sem, x_own, x_send, x_recv, xt_send, xt_recv, w_send, w_recv, doc_sem, rs_send, rs_recv,
    sq_send, sq_recv, tip_send, tip_recv, tail_sem, end_send, end_recv, ag_send, ag_recv, tp_send, tp_recv, f_send,
    f_recv, ft_send, ft_recv,
):
    g = G
    me = lax.axis_index("sp")
    core = lax.axis_index("tp")
    outer = n_sp // g
    if square:
        inner = 2 * lax.rem(me // 4, 2) + lax.rem(me, 2)
        place = 2 * (me // 8) + lax.rem(me // 2, 2)
    else:
        inner, place = lax.rem(me, g), me // g
    near = {m: flip(inner, m) for m in (1, 2, 3)}
    at_sp = {m: member(square, place, near[m]) for m in (1, 2, 3)}
    layers, width, chans = win_in.shape
    rows, features = xbuf.shape[1], xbuf.shape[2] * g
    taps = taps_ref.shape[1]
    halves, span = hid.shape[0], hid.shape[3]
    parts = w_send.shape[1]
    wide = chans // parts
    first_parts = max(parts // halves, 1)
    half = rows // n_tp
    mine = pl.ds(core * half, half)
    strided = len(x_in.shape) == 2
    pieces = outer if strided else 1
    after = lax.rem(me + 1, n_sp)
    not_last, not_first = me < n_sp - 1, me > 0

    def ways(share, l):
        cut = int(rows * share[min(l, 1)]) // 16 * 16
        return pl.ds(0, cut), pl.ds(cut, rows - cut)

    def piece(ref, at, j, o):
        if strided:
            return ref.at[at, pl.ds(pl.multiple_of(member(square, o, j) * width, width), width)]
        return ref.at[j, at, :]

    def slot(ref, j, at, o):
        return ref.at[j, at, pl.ds(o * width, width)] if strided else ref.at[j, at, :]

    def wref(l, kind, q):
        if kind == 0:
            return win_in.at[l, :, pl.ds(q * wide, wide)]
        return wout_in.at[l, pl.ds(q * wide, wide), :]

    def wslot(l, kind, q, o):
        if kind == 0:
            return win.at[l, pl.ds(o * width, width), pl.ds(q * wide, wide)]
        return wout.at[l, o, pl.ds(q * wide, wide), :]

    def weight_own(l, kind, q):
        return pltpu.make_async_copy(
            wref(l, kind, q), wslot(l, kind, q, place), own_sem.at[2 * l + kind, q]
        )

    def weight_copy(l, kind, q, to, src, o, sem, landed):
        k = 2 * l + kind
        return send(
            src, wslot(l, kind, q, o), w_send.at[k, q, sem], w_recv.at[k, q, landed],
            sp=member(square, to, inner),
        )

    def weight_copies(l, kind, q):
        own = wref(l, kind, q)
        if square:
            return [
                weight_copy(l, kind, q, flip(place, m), own, place, s, s)
                for s, m in enumerate((2, 1))
            ]
        copies = []
        for step in range(1, outer):
            to = lax.rem(place + step, outer)
            copies.append(weight_copy(l, kind, q, to, own, place, to, place))
        return copies

    def weight_go(l, kind, q, which=None):
        if q < parts and l < layers:
            for s, copy in enumerate(weight_copies(l, kind, q)):
                if which in (None, s) or not square:
                    copy.start()

    def weight_forward(l, kind, q):
        o = flip(place, 2)
        return weight_copy(l, kind, q, flip(place, 1), wslot(l, kind, q, o), o, 2, 2)

    def weight_arrived(l, kind, q, o, sem):
        weight_copy(l, kind, q, flip(place, 1), wslot(l, kind, q, o), o, 0, sem).wait_recv()

    def weight_relay(l, kind, q):
        if square and q < parts and l < layers:
            weight_arrived(l, kind, q, flip(place, 2), 0)
            weight_forward(l, kind, q).start()

    def weight_wait(l, kind, h):
        for q in range(h * parts // halves, (h + 1) * parts // halves):
            part_wait(l, kind, q)

    def part_wait(l, kind, q):
        weight_own(l, kind, q).wait()
        if square:
            weight_arrived(l, kind, q, flip(place, 1), 1)
            weight_arrived(l, kind, q, flip(place, 3), 2)
        else:
            for step in range(1, outer):
                o = lax.rem(place + step, outer)
                src = wref(l, kind, q)
                weight_copy(l, kind, q, o, src, o, o, o).wait_recv()

    def weight_close(l, kind, q):
        for copy in weight_copies(l, kind, q):
            copy.wait_send()
        if square:
            weight_forward(l, kind, q).wait_send()

    def weights(l, point):
        for at, copy, ahead, kind, q in PLAN[min(l, len(PLAN) - 1)]:
            if at == point:
                (weight_go if copy == "go" else weight_relay)(l + ahead, kind, q)

    def x_copy(m, o, landed):
        j = flip(inner, m)
        return send(
            piece(x_in, mine, j, o),
            slot(xbuf, landed, mine, o),
            x_send.at[m, o],
            x_recv.at[m, o],
            sp=member(square, place, j),
        )

    def own_piece(o):
        everything = pl.ds(0, rows)
        return pltpu.make_async_copy(
            piece(x_in, everything, inner, o), slot(xbuf, inner, everything, o), x_own.at[o]
        )

    barrier = pltpu.get_barrier_semaphore()
    greeted = [dict(sp=at_sp[m]) for m in (1, 2, 3)]
    if square:
        greeted += [dict(sp=member(square, flip(place, m), inner)) for m in (1, 2)]
    else:
        for step in range(1, outer):
            greeted.append(dict(sp=member(square, lax.rem(place + step, outer), inner)))
    for other in range(1, n_tp):
        greeted.append(dict(tp=lax.rem(core + other, n_tp)))
    for device in greeted:
        pl.semaphore_signal(barrier, inc=1, device_id=device, device_id_type=MESH)
    pl.semaphore_wait(barrier, len(greeted))

    for q in range(first_parts):
        weight_go(0, 0, q)

    def x_go(step, _):
        for o in range(pieces):
            x_copy(g - step, o, inner).start()
        return 0

    lax.fori_loop(1, g, x_go, 0)
    if square:
        for q in range(first_parts, parts):
            weight_go(0, 0, q, 1)
    for o in range(pieces):
        own_piece(o).start()
    for l in range(layers):
        for kind in range(2):
            for q in range(parts):
                weight_own(l, kind, q).start()

    column = jnp.broadcast_to(doc_ref[...].astype(F32), (128, rows))
    docs[pl.ds(8, rows), :] = jnp.transpose(column)
    doc_copy = send(
        docs.at[pl.ds(rows, 8)], doc_tail, doc_sem.at[0], doc_sem.at[1], sp=after
    )

    @pl.when(me == 0)
    def _():
        doc_tail[...] = jnp.full(doc_tail.shape, -1.0, F32)
        tails[...] = jnp.zeros(tails.shape, BF16)

    coef[...] = -RG_C * jax.nn.softplus(-decay_ref[...])
    if strided:
        for o in range(outer):
            at = pl.ds(pl.multiple_of(member(square, o, inner) * width, width), width)
            gain[:, pl.ds(o * width, width)] = gain_ref[:, at]
    else:
        gain[...] = gain_ref[...]

    def x_share(j, other, at):
        peer = lax.rem(core + other, n_tp)
        return send(
            xbuf.at[j, at], xbuf.at[j, at], xt_send.at[j, other - 1],
            xt_recv.at[j, n_tp - other - 1], tp=peer,
        )

    def x_arrive(m, _):
        j = flip(inner, m)
        for o in range(pieces):
            x_copy(m, o, j).wait_recv()
        for other in range(1, n_tp):
            x_share(j, other, mine).start()
        return 0

    for q in range(first_parts):
        weight_relay(0, 0, q)
    for q in range(first_parts, parts):
        weight_go(0, 0, q, 0)
    lax.fori_loop(1, g, x_arrive, 0)
    for o in range(pieces):
        own_piece(o).wait()

    def x_shared(m, _):
        j = flip(inner, m)
        for other in range(1, n_tp):
            peer = lax.rem(core + other, n_tp)
            at = pl.ds(peer * half, half)
            send(
                xbuf.at[j, at], xbuf.at[j, at], xt_send.at[j, other - 1],
                xt_recv.at[j, other - 1], tp=peer,
            ).wait_recv()
            x_share(j, other, mine).wait_send()
        for o in range(pieces):
            x_copy(m, o, inner).wait_send()
        return 0

    lax.fori_loop(1, g, x_shared, 0)
    for q in range(first_parts, parts - 1):
        weight_relay(0, 0, q)

    pair = 128
    dim = rgate_ref.shape[2]
    repeat = (
        lax.rem(lax.broadcasted_iota(jnp.int32, (dim, pair), 1), dim)
        == lax.broadcasted_iota(jnp.int32, (dim, pair), 0)
    ).astype(F32).astype(BF16)
    on_block = (
        lax.broadcasted_iota(jnp.int32, (pair, pair), 0) // dim
        == lax.broadcasted_iota(jnp.int32, (pair, pair), 1) // dim
    )

    def diagonal(ref, l, col):
        wide = jnp.dot(ref[l, pl.ds(col, pair), :], repeat, preferred_element_type=F32)
        return jnp.where(on_block, wide, 0.0).astype(BF16)

    sub = rows // 8
    lanes = span // pair

    def rs_copy(l, h, s):
        r0, r1 = ways(SUM_WAY, l)
        j, at, lands, to = (
            (3, r0, 2, 1), (3, r1, 2, 2), (1, r0, 0, 1), (2, r1, 1, 2), (2, r0, 1, 2),
            (1, r1, 0, 1),
        )[s]
        return send(
            part.at[h, near[j], at], gotten.at[h, lands, at], rs_send.at[h, s],
            rs_recv.at[h, s], sp=at_sp[to],
        )

    def ag_copy(l, h, s):
        r0, r1 = ways(GATHER_WAY, l)
        j, at, to = (
            (0, r0, 1), (0, r1, 2), (0, r1, 1), (0, r0, 2), (1, r0, 2), (2, r1, 1),
        )[s]
        ref = hid.at[h, near[j] if j else inner, at]
        return send(ref, ref, ag_send.at[h, s], ag_recv.at[h, s], sp=at_sp[to])

    def ag_arrived(l, h, s):
        r0, r1 = ways(GATHER_WAY, l)
        j, at = ((1, r0), (2, r1), (1, r1), (2, r0), (3, r0), (3, r1))[s]
        ref = hid.at[h, near[j], at]
        send(ref, ref, ag_send.at[h, s], ag_recv.at[h, s], sp=at_sp[1]).wait_recv()

    def f_copy(m, o, src, landed):
        return send(
            slot(xbuf, src, mine, o), piece(o_ref, mine, landed, o), f_send.at[m, o],
            f_recv.at[m, o], sp=member(square, place, flip(inner, m)),
        )

    def sq_copy(l, m):
        return send(
            sq_out.at[near[m]], sq_got.at[m - 1], sq_send.at[m - 1], sq_recv.at[m - 1],
            sp=at_sp[m],
        )

    def tip_copy(h, m):
        return send(
            tip_out.at[h, near[m]], tip_got.at[h, m - 1], tip_send.at[h, m - 1],
            tip_recv.at[h, m - 1], sp=at_sp[m],
        )

    def ag_close(l):
        for h in range(halves):
            for s in range(6):
                ag_copy(l, h, s).wait_send()

    tail_copies = [[] for _ in range(layers)]
    for l in range(layers):
        last = l == layers - 1

        r0, r1 = ways(SUM_WAY, l)
        weights_at = functools.partial(weights, l)

        def rs_relay(h):
            rs_copy(l, h, 0).wait_recv()
            part[h, near[2], r0] = (
                part[h, near[2], r0].astype(F32) + gotten[h, 2, r0].astype(F32)
            ).astype(BF16)
            rs_copy(l, h, 4).start()
            rs_copy(l, h, 1).wait_recv()
            part[h, near[1], r1] = (
                part[h, near[1], r1].astype(F32) + gotten[h, 2, r1].astype(F32)
            ).astype(BF16)
            rs_copy(l, h, 5).start()

        def prepare(step, _):
            m = jnp.where(step < 2, 3 - 2 * step, 6 - 2 * step)
            j = flip(inner, m)
            x = xbuf[j].astype(F32)
            squares = jnp.sum(x * x, axis=1, keepdims=True)
            sq_out[j] = jnp.transpose(jnp.broadcast_to(squares, (rows, 128)))[0:8]
            for n in (1, 2, 3):
                pl.when(m == n)(sq_copy(l, n).start)
            normed = (x * gain[l : l + 1, :]).astype(BF16)
            psend[j] = normed
            tip_in[j] = normed[rows - TAIL :]
            return 0

        lax.fori_loop(0, g, prepare, 0)
        scale = []
        prefixes = []

        def tail(h):
            if h == 0:
                for m in (1, 2, 3):
                    sq_copy(l, m).wait_recv()
                total = sq_out[inner] + sq_got[0] + sq_got[1] + sq_got[2]
                factor = lax.rsqrt(total * (1.0 / features) + EPS)[0:1]
                scale.append(jnp.transpose(jnp.broadcast_to(factor, (128, rows))))
            for m in (1, 2, 3):
                tip_copy(h, m).wait_recv()
            for c in range(lanes):
                here = pl.ds(c * pair, pair)
                total = tip_out[h, inner, :, here].astype(F32)
                for m in range(3):
                    total = total + tip_got[h, m, :, here].astype(F32)
                tail_out[l, h, :, here] = (total * scale[0][rows - TAIL :]).astype(BF16)
            tail_copy = send(
                tail_out.at[l, h], tails.at[l, h], tail_sem.at[l, h, 0], tail_sem.at[l, h, 1],
                sp=after,
            )
            pl.when(not_last)(tail_copy.start)
            tail_copies[l].append(tail_copy)

        for h in range(halves):
            weight_wait(l, 0, h)
            if l == 0 and h == 0:
                pl.when(not_last)(doc_copy.start)
            tips = tip_in[...].reshape(g * TAIL, -1)
            tips = jnp.dot(
                tips, win[l, :, h * span : (h + 1) * span], preferred_element_type=F32
            )
            tip_out[h] = tips.astype(BF16).reshape(g, TAIL, span)
            for m in (1, 2, 3):
                tip_copy(h, m).start()

            def project(step, _):
                m = jnp.where(step < 2, 3 - 2 * step, 6 - 2 * step)
                j = flip(inner, m)
                out = jnp.dot(
                    psend[j], win[l, :, h * span : (h + 1) * span], preferred_element_type=F32
                )
                part[h, j] = out.astype(BF16)

                @pl.when(step == 0)
                def _():
                    rs_copy(l, h, 0).start()
                    rs_copy(l, h, 1).start()

                pl.when(step == 1)(rs_copy(l, h, 2).start)
                pl.when(step == 2)(rs_copy(l, h, 3).start)
                return 0

            lax.fori_loop(0, g, project, 0)
            if h == 0:
                tail(h)
                if l > 0:
                    ag_close(l - 1)
                weights_at(0)
                rs_relay(0)
                weights_at(1)
        weights_at(2)

        def end_copy(h, dst, src, l=l):
            return send(
                ends.at[l, h, me], ends.at[l, h, src], end_send.at[l, h, dst],
                end_recv.at[l, h, src], sp=dst,
            )

        def collect(h):
            if l == 0 and h == 0:
                pl.when(not_first)(doc_copy.wait_recv)
                docs[pl.ds(0, 8), :] = doc_tail[...]
            for s in range(2, 6):
                rs_copy(l, h, s).wait_recv()
            for c in range(lanes):
                here = pl.ds(c * pair, pair)
                total = (
                    part[h, inner, :, here].astype(F32)
                    + gotten[h, 0, :, here].astype(F32)
                    + gotten[h, 1, :, here].astype(F32)
                )
                mixed = (total * scale[0]).astype(BF16)
                ext[pl.ds(8, rows), here] = mixed.astype(F32)

        def gates(h):
            pl.when(not_first)(tail_copies[l][h].wait_recv)
            ext[pl.ds(0, 8), :] = tails[l, h, TAIL - 8 :].astype(F32)

            for c in range(lanes):
                here = pl.ds(c * pair, pair)
                col = h * span + c * pair
                cols = pl.ds(col, pair)
                at = h * lanes + c
                row = slice(l, l + 1)
                conv = bias_ref[row, cols] + taps_ref[l, 0:1, cols] * ext[pl.ds(8, rows), here]
                for lag in range(1, taps):
                    same = docs[pl.ds(8 - lag, rows), :] == docs[pl.ds(8, rows), :]
                    shifted = ext[pl.ds(8 - lag, rows), here]
                    conv = conv + jnp.where(same, taps_ref[l, lag : lag + 1, cols] * shifted, 0.0)
                conv_out = conv.astype(BF16)
                recur = jnp.dot(conv_out, diagonal(rgate_ref, l, col), preferred_element_type=F32)
                inp = jnp.dot(conv_out, diagonal(igate_ref, l, col), preferred_element_type=F32)
                recur = jax.nn.sigmoid(recur + rbias_ref[row, cols])
                inp = jax.nn.sigmoid(inp + ibias_ref[row, cols])
                log_decay = coef[row, cols] * recur
                keep = docs[pl.ds(7, rows), :] == docs[pl.ds(8, rows), :]
                a_buf[at] = jnp.where(keep, jnp.exp(log_decay), 0.0)
                b_buf[at] = jnp.sqrt(jnp.maximum(minus_expm1(2.0 * log_decay), 0.0)) * (
                    inp * conv_out.astype(F32)
                )

            def advance(r, carry):
                at = pl.ds(r, 8, stride=sub)
                following = []
                for c in range(lanes):
                    decay, state = carry[c]
                    a = a_buf[h * lanes + c, at, :]
                    decay = decay * a
                    state = a * state + b_buf[h * lanes + c, at, :]
                    a_buf[h * lanes + c, at, :] = decay
                    b_buf[h * lanes + c, at, :] = state
                    following.append((decay, state))
                return tuple(following)

            start = (jnp.ones((8, pair), F32), jnp.zeros((8, pair), F32))
            chunks = lax.fori_loop(0, sub, advance, (start,) * lanes, unroll=4)
            decay = jnp.concatenate([c[0] for c in chunks], axis=1)
            state = jnp.concatenate([c[1] for c in chunks], axis=1)
            prefix = [(jnp.ones((1, span), F32), jnp.zeros((1, span), F32))]
            for s in range(8):
                d, e = prefix[-1]
                prefix.append((d * decay[s : s + 1], decay[s : s + 1] * e + state[s : s + 1]))
            prefixes.append(prefix)
            ends[l, h, me, 0:1, :] = prefix[8][0]
            ends[l, h, me, 1:2, :] = prefix[8][1]

            def end_to(dst, _):
                pl.when(dst > me)(lambda: end_copy(h, dst, me).start())
                return 0

            lax.fori_loop(0, n_sp, end_to, 0)

        def emit(h):
            def fold(src, state):
                pl.when(src < me)(lambda: end_copy(h, src, src).wait_recv())
                following = ends[l, h, src, 0:1, :] * state + ends[l, h, src, 1:2, :]
                return jnp.where(src < me, following, state)

            carried = lax.fori_loop(0, n_sp, fold, jnp.zeros((1, span), F32))
            for s in range(8):
                at = pl.ds(s * sub, sub)
                enter = prefixes[h][s][0] * carried + prefixes[h][s][1]
                for c in range(lanes):
                    one = enter[:, c * pair : (c + 1) * pair]
                    hid[h, inner, at, pl.ds(c * pair, pair)] = (
                        b_buf[h * lanes + c, at, :] + a_buf[h * lanes + c, at, :] * one
                    ).astype(BF16)
            ag_copy(l, h, 0).start()
            ag_copy(l, h, 1).start()

        def emit_rest(h):
            ag_copy(l, h, 2).start()
            ag_copy(l, h, 3).start()

        def ag_relay(h):
            ag_arrived(l, h, 0)
            ag_copy(l, h, 4).start()
            ag_arrived(l, h, 1)
            ag_copy(l, h, 5).start()

        for h in range(halves):
            collect(h)
            if h > 0:
                weights_at(5)
                emit(h - 1)
                weights_at(6)
            gates(h)
            if h > 0:
                emit_rest(h - 1)
                weights_at(7)
            else:
                weights_at(3)
            if h + 1 < halves:
                tail(h + 1)
                rs_relay(h + 1)
                weights_at(4)
            if h > 0:
                ag_relay(h - 1)
        if halves == 1:
            for point in (4, 5, 6, 7):
                weights_at(point)
        weights_at(8)
        emit(halves - 1)
        emit_rest(halves - 1)
        weights_at(9)
        for q in range(halves):
            weight_wait(l, 1, q)
        ag_relay(halves - 1)

        def tp_copy(j, other, landed):
            peer = lax.rem(core + other, n_tp)
            return send(
                psend.at[j], pgot.at[l, landed, j], tp_send.at[other - 1, j],
                tp_recv.at[l, landed, j], tp=peer,
            )

        def unproject(step):
            j = flip(inner, step)
            for s in range(2, 6):
                for h in range(halves):
                    pl.when(step == (1, 2, 3, 3)[s - 2])(functools.partial(ag_arrived, l, h, s))
            for block in range(outer):
                out = 0.0
                for h in range(halves):
                    out = out + jnp.dot(
                        hid[h, j], wout[l, block, h * span : (h + 1) * span],
                        preferred_element_type=F32,
                    )
                psend[j, :, block * width : (block + 1) * width] = out.astype(BF16)
            for other in range(1, n_tp):
                tp_copy(j, other, n_tp - other - 1).start()

        def finish(step):
            j = flip(inner, step)
            for other in range(1, n_tp):
                copy = tp_copy(j, other, other - 1)
                copy.wait_recv()
                copy.wait_send()
            at = mine if last else pl.ds(0, rows)
            summed = psend[j, at, :].astype(F32)
            for other in range(1, n_tp):
                summed = summed + pgot[l, other - 1, j, at, :].astype(F32)
            new = (xbuf[j, at, :].astype(F32) + summed).astype(BF16)
            xbuf[j, at, :] = new
            if last:

                @pl.when(step > 0)
                def _():
                    for o in range(pieces):
                        f_copy(step, o, j, inner).start()

        def both(step, _):
            pl.when(step < g)(lambda: unproject(step))
            pl.when(step > 0)(lambda: finish(step - 1))
            if square:
                pl.when(step == 1)(lambda: weights_at(10))
            return 0

        lax.fori_loop(0, g + 1, both, 0)
        if not square:
            weights_at(10)
        weights_at(11)

        for h in range(halves):
            for s in range(6):
                rs_copy(l, h, s).wait_send()
        for m in (1, 2, 3):
            sq_copy(l, m).wait_send()
            for h in range(halves):
                tip_copy(h, m).wait_send()

    def f_share(j, o, other, at, landed):
        ref = piece(o_ref, at, j, o)
        return send(
            ref, ref, ft_send.at[other - 1, j, o], ft_recv.at[landed, j, o],
            tp=lax.rem(core + other, n_tp),
        )

    def f_arrive(m, _):
        j = flip(inner, m)
        for o in range(pieces):
            pl.when(m > 0)(lambda: f_copy(m, o, j, j).wait_recv())
            for other in range(1, n_tp):
                f_share(j, o, other, mine, n_tp - other - 1).start()
        return 0

    for o in range(pieces):
        target = piece(o_ref, mine, inner, o)
        target[...] = slot(xbuf, inner, mine, o)[...]
    lax.fori_loop(0, g, f_arrive, 0)

    ag_close(layers - 1)
    pl.when(not_last)(doc_copy.wait_send)
    for l in range(layers):
        for kind in range(2):
            for q in range(parts):
                weight_close(l, kind, q)
        for tail_copy in tail_copies[l]:
            pl.when(not_last)(tail_copy.wait_send)

    def end_close(dst, _):
        @pl.when(dst > me)
        def _():
            for l in range(layers):
                for h in range(halves):
                    ref = ends.at[l, h, me]
                    send(
                        ref, ref, end_send.at[l, h, dst], end_recv.at[l, h, me], sp=dst
                    ).wait_send()

        return 0

    lax.fori_loop(0, n_sp, end_close, 0)

    def f_close(m, _):
        j = flip(inner, m)
        for o in range(pieces):
            pl.when(m > 0)(lambda: f_copy(m, o, j, inner).wait_send())
            for other in range(1, n_tp):
                peer = lax.rem(core + other, n_tp)
                f_share(j, o, other, pl.ds(peer * half, half), other - 1).wait_recv()
                f_share(j, o, other, mine, other - 1).wait_send()
        return 0

    lax.fori_loop(0, g, f_close, 0)


def per_device(
    tokens,
    documents,
    norm_gain,
    in_weight,
    conv_taps,
    conv_bias,
    recur_gate,
    input_gate,
    recur_bias,
    input_bias,
    decay_param,
    out_weight,
):
    g = G
    n_sp, n_tp = lax.axis_size("sp"), lax.axis_size("tp")
    outer = n_sp // g
    rows, features = tokens.shape
    layers, width, chans = in_weight.shape
    strided = width % 128 == 0
    square = strided and n_sp == 16
    pieces = outer if strided else 1
    part_width = outer * width
    halves = 2 if chans % 256 == 0 else 1
    span = chans // halves
    parts = 4 if chans % 512 == 0 else halves
    x, gain = tokens, norm_gain
    if not strided:
        inner = lax.rem(lax.axis_index("sp"), g)
        x = x.reshape(rows, outer, g, width).transpose(2, 0, 1, 3).reshape(g, rows, part_width)
        gain = norm_gain.reshape(layers, outer, g, width)
        gain = lax.dynamic_index_in_dim(gain, inner, 2, False).reshape(layers, part_width)
    dim = recur_gate.shape[2]
    slots = max(outer, 3)
    dma = pltpu.SemaphoreType.DMA
    any_space = pl.BlockSpec(memory_space=pl.ANY)
    others = max(n_tp - 1, 1)
    out = pl.pallas_call(
        functools.partial(whole_kernel, n_sp, n_tp, square),
        out_shape=jax.ShapeDtypeStruct(x.shape, x.dtype),
        in_specs=[any_space] * 3 + [VM] * 9,
        out_specs=VM,
        scratch_shapes=[
            pltpu.VMEM((g, rows, part_width), BF16),
            pltpu.VMEM((layers, part_width, chans), BF16),
            pltpu.VMEM((layers, outer, chans, width), BF16),
            pltpu.VMEM((halves, g, rows, span), BF16),
            pltpu.VMEM((halves, 3, rows, span), BF16),
            pltpu.VMEM((g, 8, rows), F32),
            pltpu.VMEM((3, 8, rows), F32),
            pltpu.VMEM((g, TAIL, part_width), BF16),
            pltpu.VMEM((halves, g, TAIL, span), BF16),
            pltpu.VMEM((halves, 3, TAIL, span), BF16),
            pltpu.VMEM((layers, halves, TAIL, span), BF16),
            pltpu.VMEM((layers, halves, TAIL, span), BF16),
            pltpu.VMEM((8, 128), F32),
            pltpu.VMEM((rows + 8, 128), F32),
            pltpu.VMEM((layers, part_width), F32),
            pltpu.VMEM((layers, chans), F32),
            pltpu.VMEM((rows + 8, span), F32),
            pltpu.VMEM((chans // 128, rows, 128), F32),
            pltpu.VMEM((chans // 128, rows, 128), F32),
            pltpu.VMEM((layers, halves, n_sp, 2, span), F32),
            pltpu.VMEM((halves, g, rows, span), BF16),
            pltpu.VMEM((g, rows, part_width), BF16),
            pltpu.VMEM((layers, others, g, rows, part_width), BF16),
            dma((2 * layers, parts)),
            dma((pieces,)),
            dma((g, pieces)),
            dma((g, pieces)),
            dma((g, others)),
            dma((g, others)),
            dma((2 * layers, parts, slots)),
            dma((2 * layers, parts, slots)),
            dma((2,)),
            dma((halves, 6)),
            dma((halves, 6)),
            dma((3,)),
            dma((3,)),
            dma((halves, 3)),
            dma((halves, 3)),
            dma((layers, halves, 2)),
            dma((layers, halves, n_sp)),
            dma((layers, halves, n_sp)),
            dma((halves, 6)),
            dma((halves, 6)),
            dma((others, g)),
            dma((layers, others, g)),
            dma((g, pieces)),
            dma((g, pieces)),
            dma((others, g, pieces)),
            dma((others, g, pieces)),
        ],
        compiler_params=pltpu.CompilerParams(
            has_side_effects=True, vmem_limit_bytes=60 * 1024 * 1024, collective_id=0
        ),
    )(
        x, in_weight, out_weight, documents.reshape(1, rows), gain, conv_taps, conv_bias,
        recur_bias, input_bias, decay_param,
        recur_gate.reshape(layers, chans, dim), input_gate.reshape(layers, chans, dim),
    )
    if not strided:
        out = out.reshape(g, rows, outer, width).transpose(1, 2, 0, 3).reshape(rows, features)
    return out


def solution(mesh):
    return jax.shard_map(
        per_device,
        mesh=mesh,
        in_specs=(
            P("sp", None),
            P("sp"),
            P(),
            P(None, "sp", "tp"),
            P(None, None, "tp"),
            P(None, "tp"),
            P(None, "tp", None, None),
            P(None, "tp", None, None),
            P(None, "tp"),
            P(None, "tp"),
            P(None, "tp"),
            P(None, "tp", "sp"),
        ),
        out_specs=P("sp", None),
        check_vma=False,
    )
```

```python
import functools

import jax
import jax.numpy as jnp
from jax import lax
from jax.experimental import pallas as pl
from jax.experimental.pallas import tpu as pltpu
from jax.sharding import PartitionSpec as P

RG_C = 8.0
EPS = 0.1
G = 4
SUM_WAY = (3 / 4, 5 / 8)
GATHER_WAY = (1 / 4, 3 / 8)
TAIL = 16
PLAN = (
    (
        (0, "relay", 0, 0, 3), (0, "go", 0, 1, 0), (0, "go", 0, 1, 1), (2, "go", 0, 1, 2),
        (2, "go", 0, 1, 3), (3, "relay", 0, 1, 0), (3, "relay", 0, 1, 1), (8, "relay", 0, 1, 2),
        (8, "relay", 0, 1, 3), (5, "go", 1, 0, 0), (9, "go", 1, 0, 1), (9, "go", 1, 0, 2),
        (9, "go", 1, 0, 3), (9, "relay", 1, 0, 0), (10, "relay", 1, 0, 1), (11, "relay", 1, 0, 2),
    ),
    (
        (0, "relay", 0, 0, 3), (2, "go", 0, 1, 0), (2, "go", 0, 1, 1), (3, "go", 0, 1, 2),
        (5, "go", 0, 1, 3), (4, "relay", 0, 1, 0), (7, "relay", 0, 1, 1), (8, "relay", 0, 1, 2),
        (9, "relay", 0, 1, 3),
    ),
)
MESH = pl.DeviceIdType.MESH
F32 = jnp.float32
BF16 = jnp.bfloat16
VM = pl.BlockSpec(memory_space=pltpu.VMEM)


def send(src, dst, send_sem, recv_sem, **device):
    return pltpu.make_async_remote_copy(
        src_ref=src,
        dst_ref=dst,
        send_sem=send_sem,
        recv_sem=recv_sem,
        device_id=device,
        device_id_type=MESH,
    )


def minus_expm1(x):
    series = 1.0 + x * (1.0 / 8.0)
    for n in range(7, 1, -1):
        series = 1.0 + (x * (1.0 / n)) * series
    return jnp.where(x > -0.5, -x * series, 1.0 - jnp.exp(x))


def flip(i, m):
    return 2 * lax.rem(i // 2 + m // 2, 2) + lax.rem(i + m, 2)


def member(square, o, j):
    if square:
        return (o // 2) * 8 + (j // 2) * 4 + (o % 2) * 2 + j % 2
    return o * G + j


def whole_kernel(
    n_sp, n_tp, square,
    x_in, win_in, wout_in, doc_ref, gain_ref, taps_ref, bias_ref, rbias_ref, ibias_ref, decay_ref,
    rgate_ref, igate_ref,
    o_ref,
    xbuf, win, wout, part, gotten, sq_out, sq_got, tip_in, tip_out, tip_got, tails, tail_out, doc_tail, docs, gain, coef,
    ext, a_buf, b_buf, ends, hid, psend, pgot,
    own_sem, x_own, x_send, x_recv, xt_send, xt_recv, w_send, w_recv, doc_sem, rs_send, rs_recv,
    sq_send, sq_recv, tip_send, tip_recv, tail_sem, end_send, end_recv, ag_send, ag_recv, tp_send, tp_recv, f_send,
    f_recv, ft_send, ft_recv,
):
    g = G
    me = lax.axis_index("sp")
    core = lax.axis_index("tp")
    outer = n_sp // g
    if square:
        inner = 2 * lax.rem(me // 4, 2) + lax.rem(me, 2)
        place = 2 * (me // 8) + lax.rem(me // 2, 2)
    else:
        inner, place = lax.rem(me, g), me // g
    near = {m: flip(inner, m) for m in (1, 2, 3)}
    at_sp = {m: member(square, place, near[m]) for m in (1, 2, 3)}
    layers, width, chans = win_in.shape
    rows, features = xbuf.shape[1], xbuf.shape[2] * g
    taps = taps_ref.shape[1]
    halves, span = hid.shape[0], hid.shape[3]
    parts = w_send.shape[1]
    wide = chans // parts
    first_parts = max(parts // halves, 1)
    half = rows // n_tp
    mine = pl.ds(core * half, half)
    strided = len(x_in.shape) == 2
    pieces = outer if strided else 1
    after = lax.rem(me + 1, n_sp)
    not_last, not_first = me < n_sp - 1, me > 0

    def ways(share, l):
        cut = int(rows * share[min(l, 1)]) // 16 * 16
        return pl.ds(0, cut), pl.ds(cut, rows - cut)

    def piece(ref, at, j, o):
        if strided:
            return ref.at[at, pl.ds(pl.multiple_of(member(square, o, j) * width, width), width)]
        return ref.at[j, at, :]

    def slot(ref, j, at, o):
        return ref.at[j, at, pl.ds(o * width, width)] if strided else ref.at[j, at, :]

    def wref(l, kind, q):
        if kind == 0:
            return win_in.at[l, :, pl.ds(q * wide, wide)]
        return wout_in.at[l, pl.ds(q * wide, wide), :]

    def wslot(l, kind, q, o):
        if kind == 0:
            return win.at[l, pl.ds(o * width, width), pl.ds(q * wide, wide)]
        return wout.at[l, o, pl.ds(q * wide, wide), :]

    def weight_own(l, kind, q):
        return pltpu.make_async_copy(
            wref(l, kind, q), wslot(l, kind, q, place), own_sem.at[2 * l + kind, q]
        )

    def weight_copy(l, kind, q, to, src, o, sem, landed):
        k = 2 * l + kind
        return send(
            src, wslot(l, kind, q, o), w_send.at[k, q, sem], w_recv.at[k, q, landed],
            sp=member(square, to, inner),
        )

    def weight_copies(l, kind, q):
        own = wref(l, kind, q)
        if square:
            return [
                weight_copy(l, kind, q, flip(place, m), own, place, s, s)
                for s, m in enumerate((2, 1))
            ]
        copies = []
        for step in range(1, outer):
            to = lax.rem(place + step, outer)
            copies.append(weight_copy(l, kind, q, to, own, place, to, place))
        return copies

    def weight_go(l, kind, q, which=None):
        if q < parts and l < layers:
            for s, copy in enumerate(weight_copies(l, kind, q)):
                if which in (None, s) or not square:
                    copy.start()

    def weight_forward(l, kind, q):
        o = flip(place, 2)
        return weight_copy(l, kind, q, flip(place, 1), wslot(l, kind, q, o), o, 2, 2)

    def weight_arrived(l, kind, q, o, sem):
        weight_copy(l, kind, q, flip(place, 1), wslot(l, kind, q, o), o, 0, sem).wait_recv()

    def weight_relay(l, kind, q):
        if square and q < parts and l < layers:
            weight_arrived(l, kind, q, flip(place, 2), 0)
            weight_forward(l, kind, q).start()

    def weight_wait(l, kind, h):
        for q in range(h * parts // halves, (h + 1) * parts // halves):
            part_wait(l, kind, q)

    def part_wait(l, kind, q):
        weight_own(l, kind, q).wait()
        if square:
            weight_arrived(l, kind, q, flip(place, 1), 1)
            weight_arrived(l, kind, q, flip(place, 3), 2)
        else:
            for step in range(1, outer):
                o = lax.rem(place + step, outer)
                src = wref(l, kind, q)
                weight_copy(l, kind, q, o, src, o, o, o).wait_recv()

    def weight_close(l, kind, q):
        for copy in weight_copies(l, kind, q):
            copy.wait_send()
        if square:
            weight_forward(l, kind, q).wait_send()

    def weights(l, point):
        for at, copy, ahead, kind, q in PLAN[min(l, len(PLAN) - 1)]:
            if at == point:
                (weight_go if copy == "go" else weight_relay)(l + ahead, kind, q)

    def x_copy(m, o, landed):
        j = flip(inner, m)
        return send(
            piece(x_in, mine, j, o),
            slot(xbuf, landed, mine, o),
            x_send.at[m, o],
            x_recv.at[m, o],
            sp=member(square, place, j),
        )

    def own_piece(o):
        everything = pl.ds(0, rows)
        return pltpu.make_async_copy(
            piece(x_in, everything, inner, o), slot(xbuf, inner, everything, o), x_own.at[o]
        )

    barrier = pltpu.get_barrier_semaphore()
    greeted = [dict(sp=at_sp[m]) for m in (1, 2, 3)]
    if square:
        greeted += [dict(sp=member(square, flip(place, m), inner)) for m in (1, 2)]
    else:
        for step in range(1, outer):
            greeted.append(dict(sp=member(square, lax.rem(place + step, outer), inner)))
    for other in range(1, n_tp):
        greeted.append(dict(tp=lax.rem(core + other, n_tp)))
    for device in greeted:
        pl.semaphore_signal(barrier, inc=1, device_id=device, device_id_type=MESH)
    pl.semaphore_wait(barrier, len(greeted))

    for q in range(first_parts):
        weight_go(0, 0, q)

    def x_go(step, _):
        for o in range(pieces):
            x_copy(g - step, o, inner).start()
        return 0

    lax.fori_loop(1, g, x_go, 0)
    if square:
        for q in range(first_parts, parts):
            weight_go(0, 0, q, 1)
    for o in range(pieces):
        own_piece(o).start()
    for l in range(layers):
        for kind in range(2):
            for q in range(parts):
                weight_own(l, kind, q).start()

    column = jnp.broadcast_to(doc_ref[...].astype(F32), (128, rows))
    docs[pl.ds(8, rows), :] = jnp.transpose(column)
    doc_copy = send(
        docs.at[pl.ds(rows, 8)], doc_tail, doc_sem.at[0], doc_sem.at[1], sp=after
    )

    @pl.when(me == 0)
    def _():
        doc_tail[...] = jnp.full(doc_tail.shape, -1.0, F32)
        tails[...] = jnp.zeros(tails.shape, BF16)

    coef[...] = -RG_C * jax.nn.softplus(-decay_ref[...])
    if strided:
        for o in range(outer):
            at = pl.ds(pl.multiple_of(member(square, o, inner) * width, width), width)
            gain[:, pl.ds(o * width, width)] = gain_ref[:, at]
    else:
        gain[...] = gain_ref[...]

    def x_share(j, other, at):
        peer = lax.rem(core + other, n_tp)
        return send(
            xbuf.at[j, at], xbuf.at[j, at], xt_send.at[j, other - 1],
            xt_recv.at[j, n_tp - other - 1], tp=peer,
        )

    def x_arrive(m, _):
        j = flip(inner, m)
        for o in range(pieces):
            x_copy(m, o, j).wait_recv()
        for other in range(1, n_tp):
            x_share(j, other, mine).start()
        return 0

    for q in range(first_parts):
        weight_relay(0, 0, q)
    for q in range(first_parts, parts):
        weight_go(0, 0, q, 0)
    lax.fori_loop(1, g, x_arrive, 0)
    for o in range(pieces):
        own_piece(o).wait()

    def prepare(l, m):
        j = flip(inner, m)
        x = xbuf[j].astype(F32)
        squares = jnp.sum(x * x, axis=1, keepdims=True)
        sq_out[j] = jnp.transpose(jnp.broadcast_to(squares, (rows, 128)))[0:8]
        for n in (1, 2, 3):
            pl.when(m == n)(lambda: sq_copy(l, n).start())
        normed = (x * gain[l : l + 1, :]).astype(BF16)
        psend[j] = normed
        tip_in[j] = normed[rows - TAIL :]

    def sq_copy(l, m):
        return send(
            sq_out.at[near[m]], sq_got.at[m - 1], sq_send.at[m - 1], sq_recv.at[m - 1],
            sp=at_sp[m],
        )

    prepare(0, 0)

    def x_shared(m, _):
        j = flip(inner, m)
        for other in range(1, n_tp):
            peer = lax.rem(core + other, n_tp)
            at = pl.ds(peer * half, half)
            send(
                xbuf.at[j, at], xbuf.at[j, at], xt_send.at[j, other - 1],
                xt_recv.at[j, other - 1], tp=peer,
            ).wait_recv()
            x_share(j, other, mine).wait_send()
        for o in range(pieces):
            x_copy(m, o, inner).wait_send()
        prepare(0, m)
        return 0

    lax.fori_loop(1, g, x_shared, 0)
    for q in range(first_parts, parts - 1):
        weight_relay(0, 0, q)

    pair = 128
    dim = rgate_ref.shape[2]
    repeat = (
        lax.rem(lax.broadcasted_iota(jnp.int32, (dim, pair), 1), dim)
        == lax.broadcasted_iota(jnp.int32, (dim, pair), 0)
    ).astype(F32).astype(BF16)
    on_block = (
        lax.broadcasted_iota(jnp.int32, (pair, pair), 0) // dim
        == lax.broadcasted_iota(jnp.int32, (pair, pair), 1) // dim
    )

    def diagonal(ref, l, col):
        wide = jnp.dot(ref[l, pl.ds(col, pair), :], repeat, preferred_element_type=F32)
        return jnp.where(on_block, wide, 0.0).astype(BF16)

    sub = rows // 8
    lanes = span // pair

    def rs_copy(l, h, s):
        r0, r1 = ways(SUM_WAY, l)
        j, at, lands, to = (
            (3, r0, 2, 1), (3, r1, 2, 2), (1, r0, 0, 1), (2, r1, 1, 2), (2, r0, 1, 2),
            (1, r1, 0, 1),
        )[s]
        return send(
            part.at[h, near[j], at], gotten.at[h, lands, at], rs_send.at[h, s],
            rs_recv.at[h, s], sp=at_sp[to],
        )

    def ag_copy(l, h, s):
        r0, r1 = ways(GATHER_WAY, l)
        j, at, to = (
            (0, r0, 1), (0, r1, 2), (0, r1, 1), (0, r0, 2), (1, r0, 2), (2, r1, 1),
        )[s]
        ref = hid.at[h, near[j] if j else inner, at]
        return send(ref, ref, ag_send.at[h, s], ag_recv.at[h, s], sp=at_sp[to])

    def ag_arrived(l, h, s):
        r0, r1 = ways(GATHER_WAY, l)
        j, at = ((1, r0), (2, r1), (1, r1), (2, r0), (3, r0), (3, r1))[s]
        ref = hid.at[h, near[j], at]
        send(ref, ref, ag_send.at[h, s], ag_recv.at[h, s], sp=at_sp[1]).wait_recv()

    def f_copy(m, o, src, landed):
        return send(
            slot(xbuf, src, mine, o), piece(o_ref, mine, landed, o), f_send.at[m, o],
            f_recv.at[m, o], sp=member(square, place, flip(inner, m)),
        )

    def tip_copy(h, m):
        return send(
            tip_out.at[h, near[m]], tip_got.at[h, m - 1], tip_send.at[h, m - 1],
            tip_recv.at[h, m - 1], sp=at_sp[m],
        )

    def ag_close(l):
        for h in range(halves):
            for s in range(6):
                ag_copy(l, h, s).wait_send()

    tail_copies = [[] for _ in range(layers)]
    for l in range(layers):
        last = l == layers - 1

        r0, r1 = ways(SUM_WAY, l)
        weights_at = functools.partial(weights, l)

        def rs_relay(h):
            rs_copy(l, h, 0).wait_recv()
            part[h, near[2], r0] = (
                part[h, near[2], r0].astype(F32) + gotten[h, 2, r0].astype(F32)
            ).astype(BF16)
            rs_copy(l, h, 4).start()
            rs_copy(l, h, 1).wait_recv()
            part[h, near[1], r1] = (
                part[h, near[1], r1].astype(F32) + gotten[h, 2, r1].astype(F32)
            ).astype(BF16)
            rs_copy(l, h, 5).start()

        scale = []
        prefixes = []

        def tail(h):
            if h == 0:
                for m in (1, 2, 3):
                    sq_copy(l, m).wait_recv()
                total = sq_out[inner] + sq_got[0] + sq_got[1] + sq_got[2]
                factor = lax.rsqrt(total * (1.0 / features) + EPS)[0:1]
                scale.append(jnp.transpose(jnp.broadcast_to(factor, (128, rows))))
            for m in (1, 2, 3):
                tip_copy(h, m).wait_recv()
            for c in range(lanes):
                here = pl.ds(c * pair, pair)
                total = tip_out[h, inner, :, here].astype(F32)
                for m in range(3):
                    total = total + tip_got[h, m, :, here].astype(F32)
                tail_out[l, h, :, here] = (total * scale[0][rows - TAIL :]).astype(BF16)
            tail_copy = send(
                tail_out.at[l, h], tails.at[l, h], tail_sem.at[l, h, 0], tail_sem.at[l, h, 1],
                sp=after,
            )
            pl.when(not_last)(tail_copy.start)
            tail_copies[l].append(tail_copy)

        for h in range(halves):
            weight_wait(l, 0, h)
            if l == 0 and h == 0:
                pl.when(not_last)(doc_copy.start)
            tips = tip_in[...].reshape(g * TAIL, -1)
            tips = jnp.dot(
                tips, win[l, :, h * span : (h + 1) * span], preferred_element_type=F32
            )
            tip_out[h] = tips.astype(BF16).reshape(g, TAIL, span)
            for m in (1, 2, 3):
                tip_copy(h, m).start()

            def project(step, _):
                m = jnp.where(step < 2, 3 - 2 * step, 6 - 2 * step)
                j = flip(inner, m)
                out = jnp.dot(
                    psend[j], win[l, :, h * span : (h + 1) * span], preferred_element_type=F32
                )
                part[h, j] = out.astype(BF16)

                @pl.when(step == 0)
                def _():
                    rs_copy(l, h, 0).start()
                    rs_copy(l, h, 1).start()

                pl.when(step == 1)(rs_copy(l, h, 2).start)
                pl.when(step == 2)(rs_copy(l, h, 3).start)
                return 0

            lax.fori_loop(0, g, project, 0)
            if h == 0:
                tail(h)
                if l > 0:
                    ag_close(l - 1)
                weights_at(0)
                rs_relay(0)
                weights_at(1)
        weights_at(2)

        def end_copy(h, dst, src, l=l):
            return send(
                ends.at[l, h, me], ends.at[l, h, src], end_send.at[l, h, dst],
                end_recv.at[l, h, src], sp=dst,
            )

        def collect(h):
            if l == 0 and h == 0:
                pl.when(not_first)(doc_copy.wait_recv)
                docs[pl.ds(0, 8), :] = doc_tail[...]
            for s in range(2, 6):
                rs_copy(l, h, s).wait_recv()
            for c in range(lanes):
                here = pl.ds(c * pair, pair)
                total = (
                    part[h, inner, :, here].astype(F32)
                    + gotten[h, 0, :, here].astype(F32)
                    + gotten[h, 1, :, here].astype(F32)
                )
                mixed = (total * scale[0]).astype(BF16)
                ext[pl.ds(8, rows), here] = mixed.astype(F32)

        def gates(h):
            pl.when(not_first)(tail_copies[l][h].wait_recv)
            ext[pl.ds(0, 8), :] = tails[l, h, TAIL - 8 :].astype(F32)

            for c in range(lanes):
                here = pl.ds(c * pair, pair)
                col = h * span + c * pair
                cols = pl.ds(col, pair)
                at = h * lanes + c
                row = slice(l, l + 1)
                conv = bias_ref[row, cols] + taps_ref[l, 0:1, cols] * ext[pl.ds(8, rows), here]
                for lag in range(1, taps):
                    same = docs[pl.ds(8 - lag, rows), :] == docs[pl.ds(8, rows), :]
                    shifted = ext[pl.ds(8 - lag, rows), here]
                    conv = conv + jnp.where(same, taps_ref[l, lag : lag + 1, cols] * shifted, 0.0)
                conv_out = conv.astype(BF16)
                recur = jnp.dot(conv_out, diagonal(rgate_ref, l, col), preferred_element_type=F32)
                inp = jnp.dot(conv_out, diagonal(igate_ref, l, col), preferred_element_type=F32)
                recur = jax.nn.sigmoid(recur + rbias_ref[row, cols])
                inp = jax.nn.sigmoid(inp + ibias_ref[row, cols])
                log_decay = coef[row, cols] * recur
                keep = docs[pl.ds(7, rows), :] == docs[pl.ds(8, rows), :]
                a_buf[at] = jnp.where(keep, jnp.exp(log_decay), 0.0)
                b_buf[at] = jnp.sqrt(jnp.maximum(minus_expm1(2.0 * log_decay), 0.0)) * (
                    inp * conv_out.astype(F32)
                )

            def advance(r, carry):
                at = pl.ds(r, 8, stride=sub)
                following = []
                for c in range(lanes):
                    decay, state = carry[c]
                    a = a_buf[h * lanes + c, at, :]
                    decay = decay * a
                    state = a * state + b_buf[h * lanes + c, at, :]
                    a_buf[h * lanes + c, at, :] = decay
                    b_buf[h * lanes + c, at, :] = state
                    following.append((decay, state))
                return tuple(following)

            start = (jnp.ones((8, pair), F32), jnp.zeros((8, pair), F32))
            chunks = lax.fori_loop(0, sub, advance, (start,) * lanes, unroll=4)
            decay = jnp.concatenate([c[0] for c in chunks], axis=1)
            state = jnp.concatenate([c[1] for c in chunks], axis=1)
            prefix = [(jnp.ones((1, span), F32), jnp.zeros((1, span), F32))]
            for s in range(8):
                d, e = prefix[-1]
                prefix.append((d * decay[s : s + 1], decay[s : s + 1] * e + state[s : s + 1]))
            prefixes.append(prefix)
            ends[l, h, me, 0:1, :] = prefix[8][0]
            ends[l, h, me, 1:2, :] = prefix[8][1]

            def end_to(dst, _):
                pl.when(dst > me)(lambda: end_copy(h, dst, me).start())
                return 0

            lax.fori_loop(0, n_sp, end_to, 0)

        def emit(h):
            def fold(src, state):
                pl.when(src < me)(lambda: end_copy(h, src, src).wait_recv())
                following = ends[l, h, src, 0:1, :] * state + ends[l, h, src, 1:2, :]
                return jnp.where(src < me, following, state)

            carried = lax.fori_loop(0, n_sp, fold, jnp.zeros((1, span), F32))
            for s in range(8):
                at = pl.ds(s * sub, sub)
                enter = prefixes[h][s][0] * carried + prefixes[h][s][1]
                for c in range(lanes):
                    one = enter[:, c * pair : (c + 1) * pair]
                    hid[h, inner, at, pl.ds(c * pair, pair)] = (
                        b_buf[h * lanes + c, at, :] + a_buf[h * lanes + c, at, :] * one
                    ).astype(BF16)
            ag_copy(l, h, 0).start()
            ag_copy(l, h, 1).start()

        def emit_rest(h):
            ag_copy(l, h, 2).start()
            ag_copy(l, h, 3).start()

        def ag_relay(h):
            ag_arrived(l, h, 0)
            ag_copy(l, h, 4).start()
            ag_arrived(l, h, 1)
            ag_copy(l, h, 5).start()

        for h in range(halves):
            collect(h)
            if h > 0:
                weights_at(5)
                emit(h - 1)
                weights_at(6)
            gates(h)
            if h > 0:
                emit_rest(h - 1)
                weights_at(7)
            else:
                weights_at(3)
            if h + 1 < halves:
                tail(h + 1)
                rs_relay(h + 1)
                weights_at(4)
            if h > 0:
                ag_relay(h - 1)
        if halves == 1:
            for point in (4, 5, 6, 7):
                weights_at(point)
        weights_at(8)
        emit(halves - 1)
        emit_rest(halves - 1)
        weights_at(9)
        for q in range(halves):
            weight_wait(l, 1, q)
        ag_relay(halves - 1)

        def tp_copy(j, other, landed):
            peer = lax.rem(core + other, n_tp)
            return send(
                psend.at[j], pgot.at[l, landed, j], tp_send.at[other - 1, j],
                tp_recv.at[l, landed, j], tp=peer,
            )

        for m in (1, 2, 3):
            sq_copy(l, m).wait_send()

        def unproject(step):
            j = flip(inner, step)
            for s in range(2, 6):
                for h in range(halves):
                    pl.when(step == (1, 2, 3, 3)[s - 2])(functools.partial(ag_arrived, l, h, s))
            for block in range(outer):
                out = 0.0
                for h in range(halves):
                    out = out + jnp.dot(
                        hid[h, j], wout[l, block, h * span : (h + 1) * span],
                        preferred_element_type=F32,
                    )
                psend[j, :, block * width : (block + 1) * width] = out.astype(BF16)
            for other in range(1, n_tp):
                tp_copy(j, other, n_tp - other - 1).start()

        def finish(step):
            j = flip(inner, step)
            for other in range(1, n_tp):
                copy = tp_copy(j, other, other - 1)
                copy.wait_recv()
                copy.wait_send()
            at = mine if last else pl.ds(0, rows)
            summed = psend[j, at, :].astype(F32)
            for other in range(1, n_tp):
                summed = summed + pgot[l, other - 1, j, at, :].astype(F32)
            new = (xbuf[j, at, :].astype(F32) + summed).astype(BF16)
            xbuf[j, at, :] = new
            if not last:
                prepare(l + 1, step)
            else:

                @pl.when(step > 0)
                def _():
                    for o in range(pieces):
                        f_copy(step, o, j, inner).start()

        def both(step, _):
            pl.when(step < g)(lambda: unproject(step))
            pl.when(step > 0)(lambda: finish(step - 1))
            if square:
                pl.when(step == 1)(lambda: weights_at(10))
            return 0

        lax.fori_loop(0, g + 1, both, 0)
        if not square:
            weights_at(10)
        weights_at(11)

        for h in range(halves):
            for s in range(6):
                rs_copy(l, h, s).wait_send()
        for m in (1, 2, 3):
            for h in range(halves):
                tip_copy(h, m).wait_send()

    def f_share(j, o, other, at, landed):
        ref = piece(o_ref, at, j, o)
        return send(
            ref, ref, ft_send.at[other - 1, j, o], ft_recv.at[landed, j, o],
            tp=lax.rem(core + other, n_tp),
        )

    def f_arrive(m, _):
        j = flip(inner, m)
        for o in range(pieces):
            pl.when(m > 0)(lambda: f_copy(m, o, j, j).wait_recv())
            for other in range(1, n_tp):
                f_share(j, o, other, mine, n_tp - other - 1).start()
        return 0

    for o in range(pieces):
        target = piece(o_ref, mine, inner, o)
        target[...] = slot(xbuf, inner, mine, o)[...]
    lax.fori_loop(0, g, f_arrive, 0)

    ag_close(layers - 1)
    pl.when(not_last)(doc_copy.wait_send)
    for l in range(layers):
        for kind in range(2):
            for q in range(parts):
                weight_close(l, kind, q)
        for tail_copy in tail_copies[l]:
            pl.when(not_last)(tail_copy.wait_send)

    def end_close(dst, _):
        @pl.when(dst > me)
        def _():
            for l in range(layers):
                for h in range(halves):
                    ref = ends.at[l, h, me]
                    send(
                        ref, ref, end_send.at[l, h, dst], end_recv.at[l, h, me], sp=dst
                    ).wait_send()

        return 0

    lax.fori_loop(0, n_sp, end_close, 0)

    def f_close(m, _):
        j = flip(inner, m)
        for o in range(pieces):
            pl.when(m > 0)(lambda: f_copy(m, o, j, inner).wait_send())
            for other in range(1, n_tp):
                peer = lax.rem(core + other, n_tp)
                f_share(j, o, other, pl.ds(peer * half, half), other - 1).wait_recv()
                f_share(j, o, other, mine, other - 1).wait_send()
        return 0

    lax.fori_loop(0, g, f_close, 0)


def per_device(
    tokens,
    documents,
    norm_gain,
    in_weight,
    conv_taps,
    conv_bias,
    recur_gate,
    input_gate,
    recur_bias,
    input_bias,
    decay_param,
    out_weight,
):
    g = G
    n_sp, n_tp = lax.axis_size("sp"), lax.axis_size("tp")
    outer = n_sp // g
    rows, features = tokens.shape
    layers, width, chans = in_weight.shape
    strided = width % 128 == 0
    square = strided and n_sp == 16
    pieces = outer if strided else 1
    part_width = outer * width
    halves = 2 if chans % 256 == 0 else 1
    span = chans // halves
    parts = 4 if chans % 512 == 0 else halves
    x, gain = tokens, norm_gain
    if not strided:
        inner = lax.rem(lax.axis_index("sp"), g)
        x = x.reshape(rows, outer, g, width).transpose(2, 0, 1, 3).reshape(g, rows, part_width)
        gain = norm_gain.reshape(layers, outer, g, width)
        gain = lax.dynamic_index_in_dim(gain, inner, 2, False).reshape(layers, part_width)
    dim = recur_gate.shape[2]
    slots = max(outer, 3)
    dma = pltpu.SemaphoreType.DMA
    any_space = pl.BlockSpec(memory_space=pl.ANY)
    others = max(n_tp - 1, 1)
    out = pl.pallas_call(
        functools.partial(whole_kernel, n_sp, n_tp, square),
        out_shape=jax.ShapeDtypeStruct(x.shape, x.dtype),
        in_specs=[any_space] * 3 + [VM] * 9,
        out_specs=VM,
        scratch_shapes=[
            pltpu.VMEM((g, rows, part_width), BF16),
            pltpu.VMEM((layers, part_width, chans), BF16),
            pltpu.VMEM((layers, outer, chans, width), BF16),
            pltpu.VMEM((halves, g, rows, span), BF16),
            pltpu.VMEM((halves, 3, rows, span), BF16),
            pltpu.VMEM((g, 8, rows), F32),
            pltpu.VMEM((3, 8, rows), F32),
            pltpu.VMEM((g, TAIL, part_width), BF16),
            pltpu.VMEM((halves, g, TAIL, span), BF16),
            pltpu.VMEM((halves, 3, TAIL, span), BF16),
            pltpu.VMEM((layers, halves, TAIL, span), BF16),
            pltpu.VMEM((layers, halves, TAIL, span), BF16),
            pltpu.VMEM((8, 128), F32),
            pltpu.VMEM((rows + 8, 128), F32),
            pltpu.VMEM((layers, part_width), F32),
            pltpu.VMEM((layers, chans), F32),
            pltpu.VMEM((rows + 8, span), F32),
            pltpu.VMEM((chans // 128, rows, 128), F32),
            pltpu.VMEM((chans // 128, rows, 128), F32),
            pltpu.VMEM((layers, halves, n_sp, 2, span), F32),
            pltpu.VMEM((halves, g, rows, span), BF16),
            pltpu.VMEM((g, rows, part_width), BF16),
            pltpu.VMEM((layers, others, g, rows, part_width), BF16),
            dma((2 * layers, parts)),
            dma((pieces,)),
            dma((g, pieces)),
            dma((g, pieces)),
            dma((g, others)),
            dma((g, others)),
            dma((2 * layers, parts, slots)),
            dma((2 * layers, parts, slots)),
            dma((2,)),
            dma((halves, 6)),
            dma((halves, 6)),
            dma((3,)),
            dma((3,)),
            dma((halves, 3)),
            dma((halves, 3)),
            dma((layers, halves, 2)),
            dma((layers, halves, n_sp)),
            dma((layers, halves, n_sp)),
            dma((halves, 6)),
            dma((halves, 6)),
            dma((others, g)),
            dma((layers, others, g)),
            dma((g, pieces)),
            dma((g, pieces)),
            dma((others, g, pieces)),
            dma((others, g, pieces)),
        ],
        compiler_params=pltpu.CompilerParams(
            has_side_effects=True, vmem_limit_bytes=60 * 1024 * 1024, collective_id=0
        ),
    )(
        x, in_weight, out_weight, documents.reshape(1, rows), gain, conv_taps, conv_bias,
        recur_bias, input_bias, decay_param,
        recur_gate.reshape(layers, chans, dim), input_gate.reshape(layers, chans, dim),
    )
    if not strided:
        out = out.reshape(g, rows, outer, width).transpose(1, 2, 0, 3).reshape(rows, features)
    return out


def solution(mesh):
    return jax.shard_map(
        per_device,
        mesh=mesh,
        in_specs=(
            P("sp", None),
            P("sp"),
            P(),
            P(None, "sp", "tp"),
            P(None, None, "tp"),
            P(None, "tp"),
            P(None, "tp", None, None),
            P(None, "tp", None, None),
            P(None, "tp"),
            P(None, "tp"),
            P(None, "tp"),
            P(None, "tp", "sp"),
        ),
        out_specs=P("sp", None),
        check_vma=False,
    )
```

```python
import functools

import jax
import jax.numpy as jnp
from jax import lax
from jax.experimental import pallas as pl
from jax.experimental.pallas import tpu as pltpu
from jax.sharding import PartitionSpec as P

RG_C = 8.0
EPS = 0.1
G = 4
SUM_WAY = (0.75, 0.5)
GATHER_WAY = (0.25, 0.5)
TAIL = 16
PLAN = (
    (
        (0, "relay", 0, 0, 3), (0, "go", 0, 1, 0), (0, "go", 0, 1, 1), (2, "go", 0, 1, 2),
        (2, "go", 0, 1, 3), (3, "relay", 0, 1, 0), (3, "relay", 0, 1, 1), (8, "relay", 0, 1, 2),
        (8, "relay", 0, 1, 3), (5, "go", 1, 0, 0), (9, "go", 1, 0, 1), (9, "go", 1, 0, 2),
        (9, "go", 1, 0, 3), (9, "relay", 1, 0, 0), (10, "relay", 1, 0, 1), (11, "relay", 1, 0, 2),
    ),
    (
        (0, "relay", 0, 0, 3), (2, "go", 0, 1, 0), (2, "go", 0, 1, 1), (3, "go", 0, 1, 2),
        (5, "go", 0, 1, 3), (4, "relay", 0, 1, 0), (7, "relay", 0, 1, 1), (8, "relay", 0, 1, 2),
        (9, "relay", 0, 1, 3),
    ),
)
MESH = pl.DeviceIdType.MESH
F32 = jnp.float32
BF16 = jnp.bfloat16
VM = pl.BlockSpec(memory_space=pltpu.VMEM)


def send(src, dst, send_sem, recv_sem, **device):
    return pltpu.make_async_remote_copy(
        src_ref=src,
        dst_ref=dst,
        send_sem=send_sem,
        recv_sem=recv_sem,
        device_id=device,
        device_id_type=MESH,
    )


def minus_expm1(x):
    series = 1.0 + x * (1.0 / 8.0)
    for n in range(7, 1, -1):
        series = 1.0 + (x * (1.0 / n)) * series
    return jnp.where(x > -0.5, -x * series, 1.0 - jnp.exp(x))


def flip(i, m):
    return 2 * lax.rem(i // 2 + m // 2, 2) + lax.rem(i + m, 2)


def member(square, o, j):
    if square:
        return (o // 2) * 8 + (j // 2) * 4 + (o % 2) * 2 + j % 2
    return o * G + j


def whole_kernel(
    n_sp, n_tp, square,
    x_in, win_in, wout_in, doc_ref, gain_ref, taps_ref, bias_ref, rbias_ref, ibias_ref, decay_ref,
    rgate_ref, igate_ref,
    o_ref,
    xbuf, win, wout, part, gotten, sq_out, sq_got, tip_in, tip_out, tip_got, tails, tail_out, doc_tail, docs, gain, coef,
    ext, a_buf, b_buf, ends, hid, psend, pgot,
    own_sem, x_own, x_send, x_recv, xt_send, xt_recv, w_send, w_recv, doc_sem, rs_send, rs_recv,
    sq_send, sq_recv, tip_send, tip_recv, tail_sem, end_send, end_recv, ag_send, ag_recv, tp_send, tp_recv, f_send,
    f_recv, ft_send, ft_recv,
):
    g = G
    me = lax.axis_index("sp")
    core = lax.axis_index("tp")
    outer = n_sp // g
    if square:
        inner = 2 * lax.rem(me // 4, 2) + lax.rem(me, 2)
        place = 2 * (me // 8) + lax.rem(me // 2, 2)
    else:
        inner, place = lax.rem(me, g), me // g
    near = {m: flip(inner, m) for m in (1, 2, 3)}
    at_sp = {m: member(square, place, near[m]) for m in (1, 2, 3)}
    layers, width, chans = win_in.shape
    rows, features = xbuf.shape[1], xbuf.shape[2] * g
    taps = taps_ref.shape[1]
    halves, span = hid.shape[0], hid.shape[3]
    parts = w_send.shape[1]
    wide = chans // parts
    first_parts = max(parts // halves, 1)
    half = rows // n_tp
    mine = pl.ds(core * half, half)
    strided = len(x_in.shape) == 2
    pieces = outer if strided else 1
    after = lax.rem(me + 1, n_sp)
    not_last, not_first = me < n_sp - 1, me > 0

    def ways(share, l):
        cut = int(rows * share[min(l, 1)]) // 16 * 16
        return pl.ds(0, cut), pl.ds(cut, rows - cut)

    def piece(ref, at, j, o):
        if strided:
            return ref.at[at, pl.ds(pl.multiple_of(member(square, o, j) * width, width), width)]
        return ref.at[j, at, :]

    def slot(ref, j, at, o):
        return ref.at[j, at, pl.ds(o * width, width)] if strided else ref.at[j, at, :]

    def wref(l, kind, q):
        if kind == 0:
            return win_in.at[l, :, pl.ds(q * wide, wide)]
        return wout_in.at[l, pl.ds(q * wide, wide), :]

    def wslot(l, kind, q, o):
        if kind == 0:
            return win.at[l, pl.ds(o * width, width), pl.ds(q * wide, wide)]
        return wout.at[l, o, pl.ds(q * wide, wide), :]

    def weight_own(l, kind, q):
        return pltpu.make_async_copy(
            wref(l, kind, q), wslot(l, kind, q, place), own_sem.at[2 * l + kind, q]
        )

    def weight_copy(l, kind, q, to, src, o, sem, landed):
        k = 2 * l + kind
        return send(
            src, wslot(l, kind, q, o), w_send.at[k, q, sem], w_recv.at[k, q, landed],
            sp=member(square, to, inner),
        )

    def weight_copies(l, kind, q):
        own = wref(l, kind, q)
        if square:
            return [
                weight_copy(l, kind, q, flip(place, m), own, place, s, s)
                for s, m in enumerate((2, 1))
            ]
        copies = []
        for step in range(1, outer):
            to = lax.rem(place + step, outer)
            copies.append(weight_copy(l, kind, q, to, own, place, to, place))
        return copies

    def weight_go(l, kind, q, which=None):
        if q < parts and l < layers:
            for s, copy in enumerate(weight_copies(l, kind, q)):
                if which in (None, s) or not square:
                    copy.start()

    def weight_forward(l, kind, q):
        o = flip(place, 2)
        return weight_copy(l, kind, q, flip(place, 1), wslot(l, kind, q, o), o, 2, 2)

    def weight_arrived(l, kind, q, o, sem):
        weight_copy(l, kind, q, flip(place, 1), wslot(l, kind, q, o), o, 0, sem).wait_recv()

    def weight_relay(l, kind, q):
        if square and q < parts and l < layers:
            weight_arrived(l, kind, q, flip(place, 2), 0)
            weight_forward(l, kind, q).start()

    def weight_wait(l, kind, h):
        for q in range(h * parts // halves, (h + 1) * parts // halves):
            part_wait(l, kind, q)

    def part_wait(l, kind, q):
        weight_own(l, kind, q).wait()
        if square:
            weight_arrived(l, kind, q, flip(place, 1), 1)
            weight_arrived(l, kind, q, flip(place, 3), 2)
        else:
            for step in range(1, outer):
                o = lax.rem(place + step, outer)
                src = wref(l, kind, q)
                weight_copy(l, kind, q, o, src, o, o, o).wait_recv()

    def weight_close(l, kind, q):
        for copy in weight_copies(l, kind, q):
            copy.wait_send()
        if square:
            weight_forward(l, kind, q).wait_send()

    def weights(l, point):
        for at, copy, ahead, kind, q in PLAN[min(l, len(PLAN) - 1)]:
            if at == point:
                (weight_go if copy == "go" else weight_relay)(l + ahead, kind, q)

    def x_copy(m, o, landed):
        j = flip(inner, m)
        return send(
            piece(x_in, mine, j, o),
            slot(xbuf, landed, mine, o),
            x_send.at[m, o],
            x_recv.at[m, o],
            sp=member(square, place, j),
        )

    def own_piece(o):
        everything = pl.ds(0, rows)
        return pltpu.make_async_copy(
            piece(x_in, everything, inner, o), slot(xbuf, inner, everything, o), x_own.at[o]
        )

    barrier = pltpu.get_barrier_semaphore()
    greeted = [dict(sp=at_sp[m]) for m in (1, 2, 3)]
    if square:
        greeted += [dict(sp=member(square, flip(place, m), inner)) for m in (1, 2)]
    else:
        for step in range(1, outer):
            greeted.append(dict(sp=member(square, lax.rem(place + step, outer), inner)))
    for other in range(1, n_tp):
        greeted.append(dict(tp=lax.rem(core + other, n_tp)))
    for device in greeted:
        pl.semaphore_signal(barrier, inc=1, device_id=device, device_id_type=MESH)
    pl.semaphore_wait(barrier, len(greeted))

    for q in range(first_parts):
        weight_go(0, 0, q)

    def x_go(step, _):
        for o in range(pieces):
            x_copy(g - step, o, inner).start()
        return 0

    lax.fori_loop(1, g, x_go, 0)
    if square:
        for q in range(first_parts, parts):
            weight_go(0, 0, q, 1)
    for o in range(pieces):
        own_piece(o).start()
    for l in range(layers):
        for kind in range(2):
            for q in range(parts):
                weight_own(l, kind, q).start()

    column = jnp.broadcast_to(doc_ref[...].astype(F32), (128, rows))
    docs[pl.ds(8, rows), :] = jnp.transpose(column)
    doc_copy = send(
        docs.at[pl.ds(rows, 8)], doc_tail, doc_sem.at[0], doc_sem.at[1], sp=after
    )

    @pl.when(me == 0)
    def _():
        doc_tail[...] = jnp.full(doc_tail.shape, -1.0, F32)
        tails[...] = jnp.zeros(tails.shape, BF16)

    coef[...] = -RG_C * jax.nn.softplus(-decay_ref[...])
    if strided:
        for o in range(outer):
            at = pl.ds(pl.multiple_of(member(square, o, inner) * width, width), width)
            gain[:, pl.ds(o * width, width)] = gain_ref[:, at]
    else:
        gain[...] = gain_ref[...]

    def x_share(j, other, at):
        peer = lax.rem(core + other, n_tp)
        return send(
            xbuf.at[j, at], xbuf.at[j, at], xt_send.at[j, other - 1],
            xt_recv.at[j, n_tp - other - 1], tp=peer,
        )

    def x_arrive(m, _):
        j = flip(inner, m)
        for o in range(pieces):
            x_copy(m, o, j).wait_recv()
        for other in range(1, n_tp):
            x_share(j, other, mine).start()

    for q in range(first_parts):
        weight_relay(0, 0, q)
    for q in range(first_parts, parts):
        weight_go(0, 0, q, 0)
    for o in range(pieces):
        own_piece(o).wait()

    def prepare(l, m):
        j = flip(inner, m)
        x = xbuf[j].astype(F32)
        squares = jnp.sum(x * x, axis=1, keepdims=True)
        sq_out[j] = jnp.transpose(jnp.broadcast_to(squares, (rows, 128)))[0:8]
        for n in (1, 2, 3):
            pl.when(m == n)(lambda: sq_copy(l, n).start())
        normed = (x * gain[l : l + 1, :]).astype(BF16)
        psend[j] = normed
        tip_in[j] = normed[rows - TAIL :]

    def sq_copy(l, m):
        return send(
            sq_out.at[near[m]], sq_got.at[m - 1], sq_send.at[m - 1], sq_recv.at[m - 1],
            sp=at_sp[m],
        )

    def x_shared(m, _):
        j = flip(inner, m)
        for other in range(1, n_tp):
            peer = lax.rem(core + other, n_tp)
            at = pl.ds(peer * half, half)
            send(
                xbuf.at[j, at], xbuf.at[j, at], xt_send.at[j, other - 1],
                xt_recv.at[j, other - 1], tp=peer,
            ).wait_recv()
            x_share(j, other, mine).wait_send()
        for o in range(pieces):
            x_copy(m, o, inner).wait_send()
        prepare(0, m)

    def x_come(step, _):
        @pl.when(step < g - 1)
        def _():
            m = jnp.where(step == 0, 1, 4 - step)
            x_arrive(m, 0)

        m = jnp.where(step == 0, 0, jnp.where(step == 1, 1, 5 - step))
        pl.when(step == 0)(lambda: prepare(0, 0))
        pl.when(step > 0)(lambda: x_shared(m, 0))
        return 0

    lax.fori_loop(0, g, x_come, 0)
    for q in range(first_parts, parts - 1):
        weight_relay(0, 0, q)

    pair = 128
    dim = rgate_ref.shape[2]
    repeat = (
        lax.rem(lax.broadcasted_iota(jnp.int32, (dim, pair), 1), dim)
        == lax.broadcasted_iota(jnp.int32, (dim, pair), 0)
    ).astype(F32).astype(BF16)
    on_block = (
        lax.broadcasted_iota(jnp.int32, (pair, pair), 0) // dim
        == lax.broadcasted_iota(jnp.int32, (pair, pair), 1) // dim
    )

    def diagonal(ref, l, col):
        wide = jnp.dot(ref[l, pl.ds(col, pair), :], repeat, preferred_element_type=F32)
        return jnp.where(on_block, wide, 0.0).astype(BF16)

    sub = rows // 8
    lanes = span // pair

    def rs_copy(l, h, s):
        r0, r1 = ways(SUM_WAY, l)
        j, at, lands, to = (
            (3, r0, 2, 1), (3, r1, 2, 2), (1, r0, 0, 1), (2, r1, 1, 2), (2, r0, 1, 2),
            (1, r1, 0, 1),
        )[s]
        return send(
            part.at[h, near[j], at], gotten.at[h, lands, at], rs_send.at[h, s],
            rs_recv.at[h, s], sp=at_sp[to],
        )

    def ag_copy(l, h, s):
        r0, r1 = ways(GATHER_WAY, l)
        j, at, to = (
            (0, r0, 1), (0, r1, 2), (0, r1, 1), (0, r0, 2), (1, r0, 2), (2, r1, 1),
        )[s]
        ref = hid.at[h, near[j] if j else inner, at]
        return send(ref, ref, ag_send.at[h, s], ag_recv.at[h, s], sp=at_sp[to])

    def ag_arrived(l, h, s):
        r0, r1 = ways(GATHER_WAY, l)
        j, at = ((1, r0), (2, r1), (1, r1), (2, r0), (3, r0), (3, r1))[s]
        ref = hid.at[h, near[j], at]
        send(ref, ref, ag_send.at[h, s], ag_recv.at[h, s], sp=at_sp[1]).wait_recv()

    def f_copy(m, o, src, landed):
        return send(
            slot(xbuf, src, mine, o), piece(o_ref, mine, landed, o), f_send.at[m, o],
            f_recv.at[m, o], sp=member(square, place, flip(inner, m)),
        )

    def tip_copy(h, m):
        return send(
            tip_out.at[h, near[m]], tip_got.at[h, m - 1], tip_send.at[h, m - 1],
            tip_recv.at[h, m - 1], sp=at_sp[m],
        )

    def ag_close(l):
        for h in range(halves):
            for s in range(6):
                ag_copy(l, h, s).wait_send()

    tail_copies = [[] for _ in range(layers)]
    for l in range(layers):
        last = l == layers - 1

        r0, r1 = ways(SUM_WAY, l)
        weights_at = functools.partial(weights, l)

        def rs_relay(h):
            rs_copy(l, h, 0).wait_recv()
            part[h, near[2], r0] = (
                part[h, near[2], r0].astype(F32) + gotten[h, 2, r0].astype(F32)
            ).astype(BF16)
            rs_copy(l, h, 4).start()
            rs_copy(l, h, 1).wait_recv()
            part[h, near[1], r1] = (
                part[h, near[1], r1].astype(F32) + gotten[h, 2, r1].astype(F32)
            ).astype(BF16)
            rs_copy(l, h, 5).start()

        scale = []
        prefixes = []

        def tail(h):
            if h == 0:
                for m in (1, 2, 3):
                    sq_copy(l, m).wait_recv()
                total = sq_out[inner] + sq_got[0] + sq_got[1] + sq_got[2]
                factor = lax.rsqrt(total * (1.0 / features) + EPS)[0:1]
                scale.append(jnp.transpose(jnp.broadcast_to(factor, (128, rows))))
            for m in (1, 2, 3):
                tip_copy(h, m).wait_recv()
            for c in range(lanes):
                here = pl.ds(c * pair, pair)
                total = tip_out[h, inner, :, here].astype(F32)
                for m in range(3):
                    total = total + tip_got[h, m, :, here].astype(F32)
                tail_out[l, h, :, here] = (total * scale[0][rows - TAIL :]).astype(BF16)
            tail_copy = send(
                tail_out.at[l, h], tails.at[l, h], tail_sem.at[l, h, 0], tail_sem.at[l, h, 1],
                sp=after,
            )
            pl.when(not_last)(tail_copy.start)
            tail_copies[l].append(tail_copy)

        for h in range(halves):
            weight_wait(l, 0, h)
            if l == 0 and h == 0:
                pl.when(not_last)(doc_copy.start)
            tips = tip_in[...].reshape(g * TAIL, -1)
            tips = jnp.dot(
                tips, win[l, :, h * span : (h + 1) * span], preferred_element_type=F32
            )
            tip_out[h] = tips.astype(BF16).reshape(g, TAIL, span)
            for m in (1, 2, 3):
                tip_copy(h, m).start()

            def project(step, _):
                m = jnp.where(step < 2, 3 - 2 * step, 6 - 2 * step)
                j = flip(inner, m)
                out = jnp.dot(
                    psend[j], win[l, :, h * span : (h + 1) * span], preferred_element_type=F32
                )
                part[h, j] = out.astype(BF16)

                @pl.when(step == 0)
                def _():
                    rs_copy(l, h, 0).start()
                    rs_copy(l, h, 1).start()

                pl.when(step == 1)(rs_copy(l, h, 2).start)
                pl.when(step == 2)(rs_copy(l, h, 3).start)
                return 0

            lax.fori_loop(0, g, project, 0)
            if h == 0:
                tail(h)
                if l > 0:
                    ag_close(l - 1)
                weights_at(0)
                rs_relay(0)
                weights_at(1)
        weights_at(2)

        def end_copy(h, dst, src, l=l):
            return send(
                ends.at[l, h, me], ends.at[l, h, src], end_send.at[l, h, dst],
                end_recv.at[l, h, src], sp=dst,
            )

        def collect(h):
            if l == 0 and h == 0:
                pl.when(not_first)(doc_copy.wait_recv)
                docs[pl.ds(0, 8), :] = doc_tail[...]
            for s in range(2, 6):
                rs_copy(l, h, s).wait_recv()
            for c in range(lanes):
                here = pl.ds(c * pair, pair)
                total = (
                    part[h, inner, :, here].astype(F32)
                    + gotten[h, 0, :, here].astype(F32)
                    + gotten[h, 1, :, here].astype(F32)
                )
                mixed = (total * scale[0]).astype(BF16)
                ext[pl.ds(8, rows), here] = mixed.astype(F32)

        def gates(h):
            pl.when(not_first)(tail_copies[l][h].wait_recv)
            ext[pl.ds(0, 8), :] = tails[l, h, TAIL - 8 :].astype(F32)

            for c in range(lanes):
                here = pl.ds(c * pair, pair)
                col = h * span + c * pair
                cols = pl.ds(col, pair)
                at = h * lanes + c
                row = slice(l, l + 1)
                conv = bias_ref[row, cols] + taps_ref[l, 0:1, cols] * ext[pl.ds(8, rows), here]
                for lag in range(1, taps):
                    same = docs[pl.ds(8 - lag, rows), :] == docs[pl.ds(8, rows), :]
                    shifted = ext[pl.ds(8 - lag, rows), here]
                    conv = conv + jnp.where(same, taps_ref[l, lag : lag + 1, cols] * shifted, 0.0)
                conv_out = conv.astype(BF16)
                recur = jnp.dot(conv_out, diagonal(rgate_ref, l, col), preferred_element_type=F32)
                inp = jnp.dot(conv_out, diagonal(igate_ref, l, col), preferred_element_type=F32)
                recur = jax.nn.sigmoid(recur + rbias_ref[row, cols])
                inp = jax.nn.sigmoid(inp + ibias_ref[row, cols])
                log_decay = coef[row, cols] * recur
                keep = docs[pl.ds(7, rows), :] == docs[pl.ds(8, rows), :]
                a_buf[at] = jnp.where(keep, jnp.exp(log_decay), 0.0)
                b_buf[at] = jnp.sqrt(jnp.maximum(minus_expm1(2.0 * log_decay), 0.0)) * (
                    inp * conv_out.astype(F32)
                )

            def advance(r, carry):
                at = pl.ds(r, 8, stride=sub)
                following = []
                for c in range(lanes):
                    decay, state = carry[c]
                    a = a_buf[h * lanes + c, at, :]
                    decay = decay * a
                    state = a * state + b_buf[h * lanes + c, at, :]
                    a_buf[h * lanes + c, at, :] = decay
                    b_buf[h * lanes + c, at, :] = state
                    following.append((decay, state))
                return tuple(following)

            start = (jnp.ones((8, pair), F32), jnp.zeros((8, pair), F32))
            chunks = lax.fori_loop(0, sub, advance, (start,) * lanes, unroll=4)
            decay = jnp.concatenate([c[0] for c in chunks], axis=1)
            state = jnp.concatenate([c[1] for c in chunks], axis=1)
            prefix = [(jnp.ones((1, span), F32), jnp.zeros((1, span), F32))]
            for s in range(8):
                d, e = prefix[-1]
                prefix.append((d * decay[s : s + 1], decay[s : s + 1] * e + state[s : s + 1]))
            prefixes.append(prefix)
            ends[l, h, me, 0:1, :] = prefix[8][0]
            ends[l, h, me, 1:2, :] = prefix[8][1]

            def end_to(dst, _):
                pl.when(dst > me)(lambda: end_copy(h, dst, me).start())
                return 0

            lax.fori_loop(0, n_sp, end_to, 0)

        def emit(h):
            def fold(src, state):
                pl.when(src < me)(lambda: end_copy(h, src, src).wait_recv())
                following = ends[l, h, src, 0:1, :] * state + ends[l, h, src, 1:2, :]
                return jnp.where(src < me, following, state)

            carried = lax.fori_loop(0, n_sp, fold, jnp.zeros((1, span), F32))
            for s in range(8):
                at = pl.ds(s * sub, sub)
                enter = prefixes[h][s][0] * carried + prefixes[h][s][1]
                for c in range(lanes):
                    one = enter[:, c * pair : (c + 1) * pair]
                    hid[h, inner, at, pl.ds(c * pair, pair)] = (
                        b_buf[h * lanes + c, at, :] + a_buf[h * lanes + c, at, :] * one
                    ).astype(BF16)
            ag_copy(l, h, 0).start()
            ag_copy(l, h, 1).start()

        def emit_rest(h):
            ag_copy(l, h, 2).start()
            ag_copy(l, h, 3).start()

        def ag_relay(h):
            ag_arrived(l, h, 0)
            ag_copy(l, h, 4).start()
            ag_arrived(l, h, 1)
            ag_copy(l, h, 5).start()

        for h in range(halves):
            collect(h)
            if h > 0:
                weights_at(5)
                emit(h - 1)
                weights_at(6)
            gates(h)
            if h > 0:
                emit_rest(h - 1)
                weights_at(7)
            else:
                weights_at(3)
            if h + 1 < halves:
                tail(h + 1)
                rs_relay(h + 1)
                weights_at(4)
            if h > 0:
                ag_relay(h - 1)
        if halves == 1:
            for point in (4, 5, 6, 7):
                weights_at(point)
        weights_at(8)
        emit(halves - 1)
        emit_rest(halves - 1)
        weights_at(9)
        for q in range(halves):
            weight_wait(l, 1, q)
        ag_relay(halves - 1)

        def tp_copy(j, other, landed):
            peer = lax.rem(core + other, n_tp)
            return send(
                psend.at[j], pgot.at[l, landed, j], tp_send.at[other - 1, j],
                tp_recv.at[l, landed, j], tp=peer,
            )

        for m in (1, 2, 3):
            sq_copy(l, m).wait_send()

        def unproject(step):
            j = flip(inner, step)
            for s in range(2, 6):
                for h in range(halves):
                    pl.when(step == (1, 2, 3, 3)[s - 2])(functools.partial(ag_arrived, l, h, s))
            for block in range(outer):
                out = 0.0
                for h in range(halves):
                    out = out + jnp.dot(
                        hid[h, j], wout[l, block, h * span : (h + 1) * span],
                        preferred_element_type=F32,
                    )
                psend[j, :, block * width : (block + 1) * width] = out.astype(BF16)
            for other in range(1, n_tp):
                tp_copy(j, other, n_tp - other - 1).start()

        def finish(step):
            j = flip(inner, step)
            for other in range(1, n_tp):
                copy = tp_copy(j, other, other - 1)
                copy.wait_recv()
                copy.wait_send()
            at = mine if last else pl.ds(0, rows)
            summed = psend[j, at, :].astype(F32)
            for other in range(1, n_tp):
                summed = summed + pgot[l, other - 1, j, at, :].astype(F32)
            new = (xbuf[j, at, :].astype(F32) + summed).astype(BF16)
            xbuf[j, at, :] = new
            if not last:
                prepare(l + 1, step)
            else:

                @pl.when(step > 0)
                def _():
                    for o in range(pieces):
                        f_copy(step, o, j, inner).start()

        def both(step, _):
            pl.when(step < g)(lambda: unproject(step))
            pl.when(step > 0)(lambda: finish(step - 1))
            if square:
                pl.when(step == 1)(lambda: weights_at(10))
            return 0

        lax.fori_loop(0, g + 1, both, 0)
        if not square:
            weights_at(10)
        weights_at(11)

        for h in range(halves):
            for s in range(6):
                rs_copy(l, h, s).wait_send()
        for m in (1, 2, 3):
            for h in range(halves):
                tip_copy(h, m).wait_send()

    def f_share(j, o, other, at, landed):
        ref = piece(o_ref, at, j, o)
        return send(
            ref, ref, ft_send.at[other - 1, j, o], ft_recv.at[landed, j, o],
            tp=lax.rem(core + other, n_tp),
        )

    def f_arrive(m, _):
        j = flip(inner, m)
        for o in range(pieces):
            pl.when(m > 0)(lambda: f_copy(m, o, j, j).wait_recv())
            for other in range(1, n_tp):
                f_share(j, o, other, mine, n_tp - other - 1).start()
        return 0

    for o in range(pieces):
        target = piece(o_ref, mine, inner, o)
        target[...] = slot(xbuf, inner, mine, o)[...]
    lax.fori_loop(0, g, f_arrive, 0)

    ag_close(layers - 1)
    pl.when(not_last)(doc_copy.wait_send)
    for l in range(layers):
        for kind in range(2):
            for q in range(parts):
                weight_close(l, kind, q)
        for tail_copy in tail_copies[l]:
            pl.when(not_last)(tail_copy.wait_send)

    def end_close(dst, _):
        @pl.when(dst > me)
        def _():
            for l in range(layers):
                for h in range(halves):
                    ref = ends.at[l, h, me]
                    send(
                        ref, ref, end_send.at[l, h, dst], end_recv.at[l, h, me], sp=dst
                    ).wait_send()

        return 0

    lax.fori_loop(0, n_sp, end_close, 0)

    def f_close(m, _):
        j = flip(inner, m)
        for o in range(pieces):
            pl.when(m > 0)(lambda: f_copy(m, o, j, inner).wait_send())
            for other in range(1, n_tp):
                peer = lax.rem(core + other, n_tp)
                f_share(j, o, other, pl.ds(peer * half, half), other - 1).wait_recv()
                f_share(j, o, other, mine, other - 1).wait_send()
        return 0

    lax.fori_loop(0, g, f_close, 0)


def per_device(
    tokens,
    documents,
    norm_gain,
    in_weight,
    conv_taps,
    conv_bias,
    recur_gate,
    input_gate,
    recur_bias,
    input_bias,
    decay_param,
    out_weight,
):
    g = G
    n_sp, n_tp = lax.axis_size("sp"), lax.axis_size("tp")
    outer = n_sp // g
    rows, features = tokens.shape
    layers, width, chans = in_weight.shape
    strided = width % 128 == 0
    square = strided and n_sp == 16
    pieces = outer if strided else 1
    part_width = outer * width
    halves = 2 if chans % 256 == 0 else 1
    span = chans // halves
    parts = 4 if chans % 512 == 0 else halves
    x, gain = tokens, norm_gain
    if not strided:
        inner = lax.rem(lax.axis_index("sp"), g)
        x = x.reshape(rows, outer, g, width).transpose(2, 0, 1, 3).reshape(g, rows, part_width)
        gain = norm_gain.reshape(layers, outer, g, width)
        gain = lax.dynamic_index_in_dim(gain, inner, 2, False).reshape(layers, part_width)
    dim = recur_gate.shape[2]
    slots = max(outer, 3)
    dma = pltpu.SemaphoreType.DMA
    any_space = pl.BlockSpec(memory_space=pl.ANY)
    others = max(n_tp - 1, 1)
    out = pl.pallas_call(
        functools.partial(whole_kernel, n_sp, n_tp, square),
        out_shape=jax.ShapeDtypeStruct(x.shape, x.dtype),
        in_specs=[any_space] * 3 + [VM] * 9,
        out_specs=VM,
        scratch_shapes=[
            pltpu.VMEM((g, rows, part_width), BF16),
            pltpu.VMEM((layers, part_width, chans), BF16),
            pltpu.VMEM((layers, outer, chans, width), BF16),
            pltpu.VMEM((halves, g, rows, span), BF16),
            pltpu.VMEM((halves, 3, rows, span), BF16),
            pltpu.VMEM((g, 8, rows), F32),
            pltpu.VMEM((3, 8, rows), F32),
            pltpu.VMEM((g, TAIL, part_width), BF16),
            pltpu.VMEM((halves, g, TAIL, span), BF16),
            pltpu.VMEM((halves, 3, TAIL, span), BF16),
            pltpu.VMEM((layers, halves, TAIL, span), BF16),
            pltpu.VMEM((layers, halves, TAIL, span), BF16),
            pltpu.VMEM((8, 128), F32),
            pltpu.VMEM((rows + 8, 128), F32),
            pltpu.VMEM((layers, part_width), F32),
            pltpu.VMEM((layers, chans), F32),
            pltpu.VMEM((rows + 8, span), F32),
            pltpu.VMEM((chans // 128, rows, 128), F32),
            pltpu.VMEM((chans // 128, rows, 128), F32),
            pltpu.VMEM((layers, halves, n_sp, 2, span), F32),
            pltpu.VMEM((halves, g, rows, span), BF16),
            pltpu.VMEM((g, rows, part_width), BF16),
            pltpu.VMEM((layers, others, g, rows, part_width), BF16),
            dma((2 * layers, parts)),
            dma((pieces,)),
            dma((g, pieces)),
            dma((g, pieces)),
            dma((g, others)),
            dma((g, others)),
            dma((2 * layers, parts, slots)),
            dma((2 * layers, parts, slots)),
            dma((2,)),
            dma((halves, 6)),
            dma((halves, 6)),
            dma((3,)),
            dma((3,)),
            dma((halves, 3)),
            dma((halves, 3)),
            dma((layers, halves, 2)),
            dma((layers, halves, n_sp)),
            dma((layers, halves, n_sp)),
            dma((halves, 6)),
            dma((halves, 6)),
            dma((others, g)),
            dma((layers, others, g)),
            dma((g, pieces)),
            dma((g, pieces)),
            dma((others, g, pieces)),
            dma((others, g, pieces)),
        ],
        compiler_params=pltpu.CompilerParams(
            has_side_effects=True, vmem_limit_bytes=60 * 1024 * 1024, collective_id=0
        ),
    )(
        x, in_weight, out_weight, documents.reshape(1, rows), gain, conv_taps, conv_bias,
        recur_bias, input_bias, decay_param,
        recur_gate.reshape(layers, chans, dim), input_gate.reshape(layers, chans, dim),
    )
    if not strided:
        out = out.reshape(g, rows, outer, width).transpose(1, 2, 0, 3).reshape(rows, features)
    return out


def solution(mesh):
    return jax.shard_map(
        per_device,
        mesh=mesh,
        in_specs=(
            P("sp", None),
            P("sp"),
            P(),
            P(None, "sp", "tp"),
            P(None, None, "tp"),
            P(None, "tp"),
            P(None, "tp", None, None),
            P(None, "tp", None, None),
            P(None, "tp"),
            P(None, "tp"),
            P(None, "tp"),
            P(None, "tp", "sp"),
        ),
        out_specs=P("sp", None),
        check_vma=False,
    )
```

```python
import functools

import jax
import jax.numpy as jnp
from jax import lax
from jax.experimental import pallas as pl
from jax.experimental.pallas import tpu as pltpu
from jax.sharding import PartitionSpec as P

RG_C = 8.0
EPS = 0.1
G = 4
SUM_WAY = (0.75, 0.5)
GATHER_WAY = (0.25, 0.5)
TAIL = 16
PLAN = (
    (
        (0, "relay", 0, 0, 3), (0, "go", 0, 1, 0), (0, "go", 0, 1, 1), (2, "go", 0, 1, 2),
        (2, "go", 0, 1, 3), (3, "relay", 0, 1, 0), (3, "relay", 0, 1, 1), (8, "relay", 0, 1, 2),
        (8, "relay", 0, 1, 3), (5, "go", 1, 0, 0), (9, "go", 1, 0, 1), (9, "go", 1, 0, 2),
        (9, "go", 1, 0, 3), (9, "relay", 1, 0, 0), (10, "relay", 1, 0, 1), (11, "relay", 1, 0, 2),
    ),
    (
        (0, "relay", 0, 0, 3), (2, "go", 0, 1, 0), (2, "go", 0, 1, 1), (3, "go", 0, 1, 2),
        (5, "go", 0, 1, 3), (4, "relay", 0, 1, 0), (7, "relay", 0, 1, 1), (8, "relay", 0, 1, 2),
        (9, "relay", 0, 1, 3),
    ),
)
MESH = pl.DeviceIdType.MESH
F32 = jnp.float32
BF16 = jnp.bfloat16
VM = pl.BlockSpec(memory_space=pltpu.VMEM)


def send(src, dst, send_sem, recv_sem, **device):
    return pltpu.make_async_remote_copy(
        src_ref=src,
        dst_ref=dst,
        send_sem=send_sem,
        recv_sem=recv_sem,
        device_id=device,
        device_id_type=MESH,
    )


def minus_expm1(x):
    series = 1.0 + x * (1.0 / 8.0)
    for n in range(7, 1, -1):
        series = 1.0 + (x * (1.0 / n)) * series
    return jnp.where(x > -0.5, -x * series, 1.0 - jnp.exp(x))


def flip(i, m):
    return 2 * lax.rem(i // 2 + m // 2, 2) + lax.rem(i + m, 2)


def member(square, o, j):
    if square:
        return (o // 2) * 8 + (j // 2) * 4 + (o % 2) * 2 + j % 2
    return o * G + j


def whole_kernel(
    n_sp, n_tp, square,
    x_in, win_in, wout_in, doc_ref, gain_ref, taps_ref, bias_ref, rbias_ref, ibias_ref, decay_ref,
    rgate_ref, igate_ref,
    o_ref,
    xbuf, win, wout, part, gotten, sq_out, sq_got, tip_in, tip_out, tip_got, tails, tail_out, doc_tail, docs, gain, coef,
    ext, a_buf, b_buf, ends, hid, psend, pgot,
    own_sem, x_own, x_send, x_recv, xt_send, xt_recv, w_send, w_recv, doc_sem, rs_send, rs_recv,
    sq_send, sq_recv, tip_send, tip_recv, tail_sem, end_send, end_recv, ag_send, ag_recv, tp_send, tp_recv, f_send,
    f_recv, ft_send, ft_recv,
):
    g = G
    me = lax.axis_index("sp")
    core = lax.axis_index("tp")
    outer = n_sp // g
    if square:
        inner = 2 * lax.rem(me // 4, 2) + lax.rem(me, 2)
        place = 2 * (me // 8) + lax.rem(me // 2, 2)
    else:
        inner, place = lax.rem(me, g), me // g
    near = {m: flip(inner, m) for m in (1, 2, 3)}
    at_sp = {m: member(square, place, near[m]) for m in (1, 2, 3)}
    layers, width, chans = win_in.shape
    rows, features = xbuf.shape[1], xbuf.shape[2] * g
    taps = taps_ref.shape[1]
    halves, span = hid.shape[0], hid.shape[3]
    parts = w_send.shape[1]
    wide = chans // parts
    first_parts = max(parts // halves, 1)
    half = rows // n_tp
    mine = pl.ds(core * half, half)
    strided = len(x_in.shape) == 2
    pieces = outer if strided else 1
    after = lax.rem(me + 1, n_sp)
    not_last, not_first = me < n_sp - 1, me > 0

    def ways(share, l):
        cut = int(rows * share[min(l, 1)]) // 16 * 16
        return pl.ds(0, cut), pl.ds(cut, rows - cut)

    def piece(ref, at, j, o):
        if strided:
            return ref.at[at, pl.ds(pl.multiple_of(member(square, o, j) * width, width), width)]
        return ref.at[j, at, :]

    def slot(ref, j, at, o):
        return ref.at[j, at, pl.ds(o * width, width)] if strided else ref.at[j, at, :]

    def wref(l, kind, q):
        if kind == 0:
            return win_in.at[l, :, pl.ds(q * wide, wide)]
        return wout_in.at[l, pl.ds(q * wide, wide), :]

    def wslot(l, kind, q, o):
        if kind == 0:
            return win.at[l, pl.ds(o * width, width), pl.ds(q * wide, wide)]
        return wout.at[l, o, pl.ds(q * wide, wide), :]

    def weight_own(l, kind, q):
        return pltpu.make_async_copy(
            wref(l, kind, q), wslot(l, kind, q, place), own_sem.at[2 * l + kind, q]
        )

    def weight_copy(l, kind, q, to, src, o, sem, landed):
        k = 2 * l + kind
        return send(
            src, wslot(l, kind, q, o), w_send.at[k, q, sem], w_recv.at[k, q, landed],
            sp=member(square, to, inner),
        )

    def weight_copies(l, kind, q):
        own = wref(l, kind, q)
        if square:
            return [
                weight_copy(l, kind, q, flip(place, m), own, place, s, s)
                for s, m in enumerate((2, 1))
            ]
        copies = []
        for step in range(1, outer):
            to = lax.rem(place + step, outer)
            copies.append(weight_copy(l, kind, q, to, own, place, to, place))
        return copies

    def weight_go(l, kind, q, which=None):
        if q < parts and l < layers:
            for s, copy in enumerate(weight_copies(l, kind, q)):
                if which in (None, s) or not square:
                    copy.start()

    def weight_forward(l, kind, q):
        o = flip(place, 2)
        return weight_copy(l, kind, q, flip(place, 1), wslot(l, kind, q, o), o, 2, 2)

    def weight_arrived(l, kind, q, o, sem):
        weight_copy(l, kind, q, flip(place, 1), wslot(l, kind, q, o), o, 0, sem).wait_recv()

    def weight_relay(l, kind, q):
        if square and q < parts and l < layers:
            weight_arrived(l, kind, q, flip(place, 2), 0)
            weight_forward(l, kind, q).start()

    def weight_wait(l, kind, h):
        for q in range(h * parts // halves, (h + 1) * parts // halves):
            part_wait(l, kind, q)

    def part_wait(l, kind, q):
        weight_own(l, kind, q).wait()
        if square:
            weight_arrived(l, kind, q, flip(place, 1), 1)
            weight_arrived(l, kind, q, flip(place, 3), 2)
        else:
            for step in range(1, outer):
                o = lax.rem(place + step, outer)
                src = wref(l, kind, q)
                weight_copy(l, kind, q, o, src, o, o, o).wait_recv()

    def weight_close(l, kind, q):
        for copy in weight_copies(l, kind, q):
            copy.wait_send()
        if square:
            weight_forward(l, kind, q).wait_send()

    def weights(l, point):
        for at, copy, ahead, kind, q in PLAN[min(l, len(PLAN) - 1)]:
            if at == point:
                (weight_go if copy == "go" else weight_relay)(l + ahead, kind, q)

    def x_copy(m, o, landed):
        j = flip(inner, m)
        return send(
            piece(x_in, mine, j, o),
            slot(xbuf, landed, mine, o),
            x_send.at[m, o],
            x_recv.at[m, o],
            sp=member(square, place, j),
        )

    def own_piece(o):
        everything = pl.ds(0, rows)
        return pltpu.make_async_copy(
            piece(x_in, everything, inner, o), slot(xbuf, inner, everything, o), x_own.at[o]
        )

    barrier = pltpu.get_barrier_semaphore()
    greeted = [dict(sp=at_sp[m]) for m in (1, 2, 3)]
    if square:
        greeted += [dict(sp=member(square, flip(place, m), inner)) for m in (1, 2)]
    else:
        for step in range(1, outer):
            greeted.append(dict(sp=member(square, lax.rem(place + step, outer), inner)))
    for other in range(1, n_tp):
        greeted.append(dict(tp=lax.rem(core + other, n_tp)))
    for device in greeted:
        pl.semaphore_signal(barrier, inc=1, device_id=device, device_id_type=MESH)
    pl.semaphore_wait(barrier, len(greeted))

    weight_go(0, 0, 0)
    for q in range(1, first_parts):
        weight_go(0, 0, q, 1)

    def x_go(step, _):
        for o in range(pieces):
            x_copy(g - step, o, inner).start()
        return 0

    lax.fori_loop(1, g, x_go, 0)
    if square:
        for q in range(1, first_parts):
            weight_go(0, 0, q, 0)
        for q in range(first_parts, parts):
            weight_go(0, 0, q, 1)
    for o in range(pieces):
        own_piece(o).start()
    for l in range(layers):
        for kind in range(2):
            for q in range(parts):
                weight_own(l, kind, q).start()

    column = jnp.broadcast_to(doc_ref[...].astype(F32), (128, rows))
    docs[pl.ds(8, rows), :] = jnp.transpose(column)
    doc_copy = send(
        docs.at[pl.ds(rows, 8)], doc_tail, doc_sem.at[0], doc_sem.at[1], sp=after
    )

    @pl.when(me == 0)
    def _():
        doc_tail[...] = jnp.full(doc_tail.shape, -1.0, F32)
        tails[...] = jnp.zeros(tails.shape, BF16)

    coef[...] = -RG_C * jax.nn.softplus(-decay_ref[...])
    if strided:
        for o in range(outer):
            at = pl.ds(pl.multiple_of(member(square, o, inner) * width, width), width)
            gain[:, pl.ds(o * width, width)] = gain_ref[:, at]
    else:
        gain[...] = gain_ref[...]

    def x_share(j, other, at):
        peer = lax.rem(core + other, n_tp)
        return send(
            xbuf.at[j, at], xbuf.at[j, at], xt_send.at[j, other - 1],
            xt_recv.at[j, n_tp - other - 1], tp=peer,
        )

    def x_arrive(m, _):
        j = flip(inner, m)
        for o in range(pieces):
            x_copy(m, o, j).wait_recv()
        for other in range(1, n_tp):
            x_share(j, other, mine).start()

    for q in range(first_parts):
        weight_relay(0, 0, q)
    for q in range(first_parts, parts):
        weight_go(0, 0, q, 0)
    for o in range(pieces):
        own_piece(o).wait()

    def prepare(l, m):
        j = flip(inner, m)
        x = xbuf[j].astype(F32)
        squares = jnp.sum(x * x, axis=1, keepdims=True)
        sq_out[j] = jnp.transpose(jnp.broadcast_to(squares, (rows, 128)))[0:8]
        for n in (1, 2, 3):
            pl.when(m == n)(lambda: sq_copy(l, n).start())
        normed = (x * gain[l : l + 1, :]).astype(BF16)
        psend[j] = normed
        tip_in[j] = normed[rows - TAIL :]

    def sq_copy(l, m):
        return send(
            sq_out.at[near[m]], sq_got.at[m - 1], sq_send.at[m - 1], sq_recv.at[m - 1],
            sp=at_sp[m],
        )

    def x_shared(m, _):
        j = flip(inner, m)
        for other in range(1, n_tp):
            peer = lax.rem(core + other, n_tp)
            at = pl.ds(peer * half, half)
            send(
                xbuf.at[j, at], xbuf.at[j, at], xt_send.at[j, other - 1],
                xt_recv.at[j, other - 1], tp=peer,
            ).wait_recv()
            x_share(j, other, mine).wait_send()
        for o in range(pieces):
            x_copy(m, o, inner).wait_send()
        prepare(0, m)

    def x_come(step, _):
        @pl.when(step < g - 1)
        def _():
            m = jnp.where(step == 0, 1, 4 - step)
            x_arrive(m, 0)

        m = jnp.where(step == 0, 0, jnp.where(step == 1, 1, 5 - step))
        pl.when(step == 0)(lambda: prepare(0, 0))
        pl.when(step > 0)(lambda: x_shared(m, 0))
        return 0

    lax.fori_loop(0, g, x_come, 0)
    for q in range(first_parts, parts - 1):
        weight_relay(0, 0, q)

    pair = 128
    dim = rgate_ref.shape[2]
    repeat = (
        lax.rem(lax.broadcasted_iota(jnp.int32, (dim, pair), 1), dim)
        == lax.broadcasted_iota(jnp.int32, (dim, pair), 0)
    ).astype(F32).astype(BF16)
    on_block = (
        lax.broadcasted_iota(jnp.int32, (pair, pair), 0) // dim
        == lax.broadcasted_iota(jnp.int32, (pair, pair), 1) // dim
    )

    def diagonal(ref, l, col):
        wide = jnp.dot(ref[l, pl.ds(col, pair), :], repeat, preferred_element_type=F32)
        return jnp.where(on_block, wide, 0.0).astype(BF16)

    sub = rows // 8
    lanes = span // pair

    def rs_copy(l, h, s):
        r0, r1 = ways(SUM_WAY, l)
        j, at, lands, to = (
            (3, r0, 2, 1), (3, r1, 2, 2), (1, r0, 0, 1), (2, r1, 1, 2), (2, r0, 1, 2),
            (1, r1, 0, 1),
        )[s]
        return send(
            part.at[h, near[j], at], gotten.at[h, lands, at], rs_send.at[h, s],
            rs_recv.at[h, s], sp=at_sp[to],
        )

    def ag_copy(l, h, s):
        r0, r1 = ways(GATHER_WAY, l)
        j, at, to = (
            (0, r0, 1), (0, r1, 2), (0, r1, 1), (0, r0, 2), (1, r0, 2), (2, r1, 1),
        )[s]
        ref = hid.at[h, near[j] if j else inner, at]
        return send(ref, ref, ag_send.at[h, s], ag_recv.at[h, s], sp=at_sp[to])

    def ag_arrived(l, h, s):
        r0, r1 = ways(GATHER_WAY, l)
        j, at = ((1, r0), (2, r1), (1, r1), (2, r0), (3, r0), (3, r1))[s]
        ref = hid.at[h, near[j], at]
        send(ref, ref, ag_send.at[h, s], ag_recv.at[h, s], sp=at_sp[1]).wait_recv()

    def f_copy(m, o, src, landed):
        return send(
            slot(xbuf, src, mine, o), piece(o_ref, mine, landed, o), f_send.at[m, o],
            f_recv.at[m, o], sp=member(square, place, flip(inner, m)),
        )

    def tip_copy(h, m):
        return send(
            tip_out.at[h, near[m]], tip_got.at[h, m - 1], tip_send.at[h, m - 1],
            tip_recv.at[h, m - 1], sp=at_sp[m],
        )

    def ag_close(l):
        for h in range(halves):
            for s in range(6):
                ag_copy(l, h, s).wait_send()

    tail_copies = [[] for _ in range(layers)]
    for l in range(layers):
        last = l == layers - 1

        r0, r1 = ways(SUM_WAY, l)
        weights_at = functools.partial(weights, l)

        def rs_relay(h):
            rs_copy(l, h, 0).wait_recv()
            part[h, near[2], r0] = (
                part[h, near[2], r0].astype(F32) + gotten[h, 2, r0].astype(F32)
            ).astype(BF16)
            rs_copy(l, h, 4).start()
            rs_copy(l, h, 1).wait_recv()
            part[h, near[1], r1] = (
                part[h, near[1], r1].astype(F32) + gotten[h, 2, r1].astype(F32)
            ).astype(BF16)
            rs_copy(l, h, 5).start()

        scale = []
        prefixes = []

        def tail(h):
            if h == 0:
                for m in (1, 2, 3):
                    sq_copy(l, m).wait_recv()
                total = sq_out[inner] + sq_got[0] + sq_got[1] + sq_got[2]
                factor = lax.rsqrt(total * (1.0 / features) + EPS)[0:1]
                scale.append(jnp.transpose(jnp.broadcast_to(factor, (128, rows))))
            for m in (1, 2, 3):
                tip_copy(h, m).wait_recv()
            for c in range(lanes):
                here = pl.ds(c * pair, pair)
                total = tip_out[h, inner, :, here].astype(F32)
                for m in range(3):
                    total = total + tip_got[h, m, :, here].astype(F32)
                tail_out[l, h, :, here] = (total * scale[0][rows - TAIL :]).astype(BF16)
            tail_copy = send(
                tail_out.at[l, h], tails.at[l, h], tail_sem.at[l, h, 0], tail_sem.at[l, h, 1],
                sp=after,
            )
            pl.when(not_last)(tail_copy.start)
            tail_copies[l].append(tail_copy)

        for h in range(halves):
            weight_wait(l, 0, h)
            if l == 0 and h == 0:
                pl.when(not_last)(doc_copy.start)
            tips = tip_in[...].reshape(g * TAIL, -1)
            tips = jnp.dot(
                tips, win[l, :, h * span : (h + 1) * span], preferred_element_type=F32
            )
            tip_out[h] = tips.astype(BF16).reshape(g, TAIL, span)
            for m in (1, 2, 3):
                tip_copy(h, m).start()

            def project(step, _):
                m = jnp.where(step < 2, 3 - 2 * step, 6 - 2 * step)
                j = flip(inner, m)
                out = jnp.dot(
                    psend[j], win[l, :, h * span : (h + 1) * span], preferred_element_type=F32
                )
                part[h, j] = out.astype(BF16)

                @pl.when(step == 0)
                def _():
                    rs_copy(l, h, 0).start()
                    rs_copy(l, h, 1).start()

                pl.when(step == 1)(rs_copy(l, h, 2).start)
                pl.when(step == 2)(rs_copy(l, h, 3).start)
                return 0

            lax.fori_loop(0, g, project, 0)
            if h == 0:
                tail(h)
                if l > 0:
                    ag_close(l - 1)
                weights_at(0)
                rs_relay(0)
                weights_at(1)
        weights_at(2)

        def end_copy(h, dst, src, l=l):
            return send(
                ends.at[l, h, me], ends.at[l, h, src], end_send.at[l, h, dst],
                end_recv.at[l, h, src], sp=dst,
            )

        def collect(h):
            if l == 0 and h == 0:
                pl.when(not_first)(doc_copy.wait_recv)
                docs[pl.ds(0, 8), :] = doc_tail[...]
            for s in range(2, 6):
                rs_copy(l, h, s).wait_recv()
            for c in range(lanes):
                here = pl.ds(c * pair, pair)
                total = (
                    part[h, inner, :, here].astype(F32)
                    + gotten[h, 0, :, here].astype(F32)
                    + gotten[h, 1, :, here].astype(F32)
                )
                mixed = (total * scale[0]).astype(BF16)
                ext[pl.ds(8, rows), here] = mixed.astype(F32)

        def gates(h):
            pl.when(not_first)(tail_copies[l][h].wait_recv)
            ext[pl.ds(0, 8), :] = tails[l, h, TAIL - 8 :].astype(F32)

            for c in range(lanes):
                here = pl.ds(c * pair, pair)
                col = h * span + c * pair
                cols = pl.ds(col, pair)
                at = h * lanes + c
                row = slice(l, l + 1)
                conv = bias_ref[row, cols] + taps_ref[l, 0:1, cols] * ext[pl.ds(8, rows), here]
                for lag in range(1, taps):
                    same = docs[pl.ds(8 - lag, rows), :] == docs[pl.ds(8, rows), :]
                    shifted = ext[pl.ds(8 - lag, rows), here]
                    conv = conv + jnp.where(same, taps_ref[l, lag : lag + 1, cols] * shifted, 0.0)
                conv_out = conv.astype(BF16)
                recur = jnp.dot(conv_out, diagonal(rgate_ref, l, col), preferred_element_type=F32)
                inp = jnp.dot(conv_out, diagonal(igate_ref, l, col), preferred_element_type=F32)
                recur = jax.nn.sigmoid(recur + rbias_ref[row, cols])
                inp = jax.nn.sigmoid(inp + ibias_ref[row, cols])
                log_decay = coef[row, cols] * recur
                keep = docs[pl.ds(7, rows), :] == docs[pl.ds(8, rows), :]
                a_buf[at] = jnp.where(keep, jnp.exp(log_decay), 0.0)
                b_buf[at] = jnp.sqrt(jnp.maximum(minus_expm1(2.0 * log_decay), 0.0)) * (
                    inp * conv_out.astype(F32)
                )

            def advance(r, carry):
                at = pl.ds(r, 8, stride=sub)
                following = []
                for c in range(lanes):
                    decay, state = carry[c]
                    a = a_buf[h * lanes + c, at, :]
                    decay = decay * a
                    state = a * state + b_buf[h * lanes + c, at, :]
                    a_buf[h * lanes + c, at, :] = decay
                    b_buf[h * lanes + c, at, :] = state
                    following.append((decay, state))
                return tuple(following)

            start = (jnp.ones((8, pair), F32), jnp.zeros((8, pair), F32))
            chunks = lax.fori_loop(0, sub, advance, (start,) * lanes, unroll=4)
            decay = jnp.concatenate([c[0] for c in chunks], axis=1)
            state = jnp.concatenate([c[1] for c in chunks], axis=1)
            prefix = [(jnp.ones((1, span), F32), jnp.zeros((1, span), F32))]
            for s in range(8):
                d, e = prefix[-1]
                prefix.append((d * decay[s : s + 1], decay[s : s + 1] * e + state[s : s + 1]))
            prefixes.append(prefix)
            ends[l, h, me, 0:1, :] = prefix[8][0]
            ends[l, h, me, 1:2, :] = prefix[8][1]

            def end_to(dst, _):
                pl.when(dst > me)(lambda: end_copy(h, dst, me).start())
                return 0

            lax.fori_loop(0, n_sp, end_to, 0)

        def emit(h):
            def fold(src, state):
                pl.when(src < me)(lambda: end_copy(h, src, src).wait_recv())
                following = ends[l, h, src, 0:1, :] * state + ends[l, h, src, 1:2, :]
                return jnp.where(src < me, following, state)

            carried = lax.fori_loop(0, n_sp, fold, jnp.zeros((1, span), F32))
            for s in range(8):
                at = pl.ds(s * sub, sub)
                enter = prefixes[h][s][0] * carried + prefixes[h][s][1]
                for c in range(lanes):
                    one = enter[:, c * pair : (c + 1) * pair]
                    hid[h, inner, at, pl.ds(c * pair, pair)] = (
                        b_buf[h * lanes + c, at, :] + a_buf[h * lanes + c, at, :] * one
                    ).astype(BF16)
            ag_copy(l, h, 0).start()
            ag_copy(l, h, 1).start()

        def emit_rest(h):
            ag_copy(l, h, 2).start()
            ag_copy(l, h, 3).start()

        def ag_relay(h):
            ag_arrived(l, h, 0)
            ag_copy(l, h, 4).start()
            ag_arrived(l, h, 1)
            ag_copy(l, h, 5).start()

        for h in range(halves):
            collect(h)
            if h > 0:
                weights_at(5)
                emit(h - 1)
                weights_at(6)
            gates(h)
            if h > 0:
                emit_rest(h - 1)
                weights_at(7)
            else:
                weights_at(3)
            if h + 1 < halves:
                tail(h + 1)
                rs_relay(h + 1)
                weights_at(4)
            if h > 0:
                ag_relay(h - 1)
        if halves == 1:
            for point in (4, 5, 6, 7):
                weights_at(point)
        weights_at(8)
        emit(halves - 1)
        emit_rest(halves - 1)
        weights_at(9)
        for q in range(halves):
            weight_wait(l, 1, q)
        ag_relay(halves - 1)

        def tp_copy(j, other, landed):
            peer = lax.rem(core + other, n_tp)
            return send(
                psend.at[j], pgot.at[l, landed, j], tp_send.at[other - 1, j],
                tp_recv.at[l, landed, j], tp=peer,
            )

        for m in (1, 2, 3):
            sq_copy(l, m).wait_send()

        def unproject(step):
            j = flip(inner, step)
            for s in range(2, 6):
                for h in range(halves):
                    pl.when(step == (1, 2, 3, 3)[s - 2])(functools.partial(ag_arrived, l, h, s))
            for block in range(outer):
                out = 0.0
                for h in range(halves):
                    out = out + jnp.dot(
                        hid[h, j], wout[l, block, h * span : (h + 1) * span],
                        preferred_element_type=F32,
                    )
                psend[j, :, block * width : (block + 1) * width] = out.astype(BF16)
            for other in range(1, n_tp):
                tp_copy(j, other, n_tp - other - 1).start()

        def finish(step):
            j = flip(inner, step)
            for other in range(1, n_tp):
                copy = tp_copy(j, other, other - 1)
                copy.wait_recv()
                copy.wait_send()
            at = mine if last else pl.ds(0, rows)
            summed = psend[j, at, :].astype(F32)
            for other in range(1, n_tp):
                summed = summed + pgot[l, other - 1, j, at, :].astype(F32)
            new = (xbuf[j, at, :].astype(F32) + summed).astype(BF16)
            xbuf[j, at, :] = new
            if not last:
                prepare(l + 1, step)
            else:

                @pl.when(step > 0)
                def _():
                    for o in range(pieces):
                        f_copy(step, o, j, inner).start()

        def both(step, _):
            pl.when(step < g)(lambda: unproject(step))
            pl.when(step > 0)(lambda: finish(step - 1))
            if square:
                pl.when(step == 1)(lambda: weights_at(10))
            return 0

        lax.fori_loop(0, g + 1, both, 0)
        if not square:
            weights_at(10)
        weights_at(11)

        for h in range(halves):
            for s in range(6):
                rs_copy(l, h, s).wait_send()
        for m in (1, 2, 3):
            for h in range(halves):
                tip_copy(h, m).wait_send()

    def f_share(j, o, other, at, landed):
        ref = piece(o_ref, at, j, o)
        return send(
            ref, ref, ft_send.at[other - 1, j, o], ft_recv.at[landed, j, o],
            tp=lax.rem(core + other, n_tp),
        )

    def f_arrive(m, _):
        j = flip(inner, m)
        for o in range(pieces):
            pl.when(m > 0)(lambda: f_copy(m, o, j, j).wait_recv())
            for other in range(1, n_tp):
                f_share(j, o, other, mine, n_tp - other - 1).start()
        return 0

    for o in range(pieces):
        target = piece(o_ref, mine, inner, o)
        target[...] = slot(xbuf, inner, mine, o)[...]
    lax.fori_loop(0, g, f_arrive, 0)

    ag_close(layers - 1)
    pl.when(not_last)(doc_copy.wait_send)
    for l in range(layers):
        for kind in range(2):
            for q in range(parts):
                weight_close(l, kind, q)
        for tail_copy in tail_copies[l]:
            pl.when(not_last)(tail_copy.wait_send)

    def end_close(dst, _):
        @pl.when(dst > me)
        def _():
            for l in range(layers):
                for h in range(halves):
                    ref = ends.at[l, h, me]
                    send(
                        ref, ref, end_send.at[l, h, dst], end_recv.at[l, h, me], sp=dst
                    ).wait_send()

        return 0

    lax.fori_loop(0, n_sp, end_close, 0)

    def f_close(m, _):
        j = flip(inner, m)
        for o in range(pieces):
            pl.when(m > 0)(lambda: f_copy(m, o, j, inner).wait_send())
            for other in range(1, n_tp):
                peer = lax.rem(core + other, n_tp)
                f_share(j, o, other, pl.ds(peer * half, half), other - 1).wait_recv()
                f_share(j, o, other, mine, other - 1).wait_send()
        return 0

    lax.fori_loop(0, g, f_close, 0)


def per_device(
    tokens,
    documents,
    norm_gain,
    in_weight,
    conv_taps,
    conv_bias,
    recur_gate,
    input_gate,
    recur_bias,
    input_bias,
    decay_param,
    out_weight,
):
    g = G
    n_sp, n_tp = lax.axis_size("sp"), lax.axis_size("tp")
    outer = n_sp // g
    rows, features = tokens.shape
    layers, width, chans = in_weight.shape
    strided = width % 128 == 0
    square = strided and n_sp == 16
    pieces = outer if strided else 1
    part_width = outer * width
    halves = 2 if chans % 256 == 0 else 1
    span = chans // halves
    parts = 4 if chans % 512 == 0 else halves
    x, gain = tokens, norm_gain
    if not strided:
        inner = lax.rem(lax.axis_index("sp"), g)
        x = x.reshape(rows, outer, g, width).transpose(2, 0, 1, 3).reshape(g, rows, part_width)
        gain = norm_gain.reshape(layers, outer, g, width)
        gain = lax.dynamic_index_in_dim(gain, inner, 2, False).reshape(layers, part_width)
    dim = recur_gate.shape[2]
    slots = max(outer, 3)
    dma = pltpu.SemaphoreType.DMA
    any_space = pl.BlockSpec(memory_space=pl.ANY)
    others = max(n_tp - 1, 1)
    out = pl.pallas_call(
        functools.partial(whole_kernel, n_sp, n_tp, square),
        out_shape=jax.ShapeDtypeStruct(x.shape, x.dtype),
        in_specs=[any_space] * 3 + [VM] * 9,
        out_specs=VM,
        scratch_shapes=[
            pltpu.VMEM((g, rows, part_width), BF16),
            pltpu.VMEM((layers, part_width, chans), BF16),
            pltpu.VMEM((layers, outer, chans, width), BF16),
            pltpu.VMEM((halves, g, rows, span), BF16),
            pltpu.VMEM((halves, 3, rows, span), BF16),
            pltpu.VMEM((g, 8, rows), F32),
            pltpu.VMEM((3, 8, rows), F32),
            pltpu.VMEM((g, TAIL, part_width), BF16),
            pltpu.VMEM((halves, g, TAIL, span), BF16),
            pltpu.VMEM((halves, 3, TAIL, span), BF16),
            pltpu.VMEM((layers, halves, TAIL, span), BF16),
            pltpu.VMEM((layers, halves, TAIL, span), BF16),
            pltpu.VMEM((8, 128), F32),
            pltpu.VMEM((rows + 8, 128), F32),
            pltpu.VMEM((layers, part_width), F32),
            pltpu.VMEM((layers, chans), F32),
            pltpu.VMEM((rows + 8, span), F32),
            pltpu.VMEM((chans // 128, rows, 128), F32),
            pltpu.VMEM((chans // 128, rows, 128), F32),
            pltpu.VMEM((layers, halves, n_sp, 2, span), F32),
            pltpu.VMEM((halves, g, rows, span), BF16),
            pltpu.VMEM((g, rows, part_width), BF16),
            pltpu.VMEM((layers, others, g, rows, part_width), BF16),
            dma((2 * layers, parts)),
            dma((pieces,)),
            dma((g, pieces)),
            dma((g, pieces)),
            dma((g, others)),
            dma((g, others)),
            dma((2 * layers, parts, slots)),
            dma((2 * layers, parts, slots)),
            dma((2,)),
            dma((halves, 6)),
            dma((halves, 6)),
            dma((3,)),
            dma((3,)),
            dma((halves, 3)),
            dma((halves, 3)),
            dma((layers, halves, 2)),
            dma((layers, halves, n_sp)),
            dma((layers, halves, n_sp)),
            dma((halves, 6)),
            dma((halves, 6)),
            dma((others, g)),
            dma((layers, others, g)),
            dma((g, pieces)),
            dma((g, pieces)),
            dma((others, g, pieces)),
            dma((others, g, pieces)),
        ],
        compiler_params=pltpu.CompilerParams(
            has_side_effects=True, vmem_limit_bytes=60 * 1024 * 1024, collective_id=0
        ),
    )(
        x, in_weight, out_weight, documents.reshape(1, rows), gain, conv_taps, conv_bias,
        recur_bias, input_bias, decay_param,
        recur_gate.reshape(layers, chans, dim), input_gate.reshape(layers, chans, dim),
    )
    if not strided:
        out = out.reshape(g, rows, outer, width).transpose(1, 2, 0, 3).reshape(rows, features)
    return out


def solution(mesh):
    return jax.shard_map(
        per_device,
        mesh=mesh,
        in_specs=(
            P("sp", None),
            P("sp"),
            P(),
            P(None, "sp", "tp"),
            P(None, None, "tp"),
            P(None, "tp"),
            P(None, "tp", None, None),
            P(None, "tp", None, None),
            P(None, "tp"),
            P(None, "tp"),
            P(None, "tp"),
            P(None, "tp", "sp"),
        ),
        out_specs=P("sp", None),
        check_vma=False,
    )
```
